32 devices in a mesh: kv: 8 (over z, x), tp: 4 (over y, core).
Axes of the slice: x: 2, y: 2, z: 4, core: 2. Of those that a mesh axis runs over, the one named last changes fastest.
Arguments:
- tokens: bfloat16 [4096, 2048], P('kv'), may hold values from -64 to 64
- query_weight: bfloat16 [2048, 2048], P(None, 'tp'), may hold values from -0.1875 to 0.1875
- chosen_key_weight: bfloat16 [2048, 512], P(None, 'tp'), may hold values from -0.125 to 0.125
- chosen_value_weight: bfloat16 [2048, 512], P(None, 'tp'), may hold values from -0.125 to 0.125
- summary_key_weight: bfloat16 [2048, 512], P(None, 'tp'), may hold values from -0.125 to 0.125
- summary_value_weight: bfloat16 [2048, 512], P(None, 'tp'), may hold values from -0.125 to 0.125
- squeeze_key_in: bfloat16 [2048, 128], replicated, may hold values from -0.125 to 0.125
- squeeze_key_out: bfloat16 [128, 64], replicated, may hold values from -1 to 1
- squeeze_value_in: bfloat16 [2048, 128], replicated, may hold values from -0.125 to 0.125
- squeeze_value_out: bfloat16 [128, 64], replicated, may hold values from -2 to 2
- gate_weight: bfloat16 [2, 2048, 32], P(None, None, 'tp'), may hold values from -0.125 to 0.125
- output_weight: bfloat16 [2048, 2048], P('tp'), may hold values from -1 to 1
- chosen_blocks: int32 [8, 128, 16], P('tp', 'kv'), may hold values from 0 to 127, as said below
Outputs:
- attended: bfloat16 [4096, 2048], P(('kv', 'tp'))
The draws below stay inside these ranges and needn't reach their ends.
Inputs may be any that keep to these rules, and one draw needn't show every extreme that they name: `chosen_blocks`: each row lists 16 different blocks. The row of query block b lists b, lists b - 1 where b > 0, and lists block 0. Take the blocks at or below their query block that the rows of the query blocks of one index of kv list for one key head: at most 4 different ones lie among the positions of any other single index of kv, and exactly 4 among the positions of the first index, for every index after the first.
All inputs are finite; a program needn't handle non-finite values.
Results may differ from the reference program's by a relative error of at most 0.03.
Values may be sent and summed in bfloat16 or wider, within the bound.
A program may use at most 128 MiB of HBM per device.

```python
import jax
import jax.numpy as jnp
from jax import lax

D = 2048
H = 32
KVH = 8
HD = 64
CMP_LEN = 32
CMP_STRIDE = 16
CMP_HIDDEN = 128
BLK = 32
NSEL = 16
CAP = 4
TOK_DEV = 512
SEQ = 4096
NB = 128
N_TP = 4


def draw_tokens(key, part):
    first, second, third = jax.random.split(key, 3)
    base = jax.random.truncated_normal(first, -4.0, 4.0, (SEQ, D), jnp.float32)
    return base.astype(jnp.bfloat16)


def draw_chosen_blocks(key, part):
    per_dev = TOK_DEV // BLK
    blocks = SEQ // BLK
    owners = blocks // per_dev
    first, second = jax.random.split(jax.random.fold_in(key, 7))
    inner = jnp.arange(per_dev, dtype=jnp.int32)
    pick = jax.random.randint(first, (KVH, owners, owners, per_dev), 0, 1 << 20) * per_dev + inner
    asker = jnp.arange(owners, dtype=jnp.int32)[:, None, None]
    holder = jnp.arange(owners, dtype=jnp.int32)[None, :, None]
    inner_row = inner[None, None, :]
    pinned = (holder == 0) & (inner_row == 0) | (holder == asker - 1) & (inner_row == per_dev - 1)
    pinned = pinned | (holder == asker - owners // 2) & (inner_row == 1)
    pick = pick + pinned.astype(jnp.int32) * (1 << 28)
    above = jnp.sum((pick[..., None, :] > pick[..., :, None]).astype(jnp.int32), -1)
    subset = above < CAP
    query_block = jnp.arange(blocks, dtype=jnp.int32)[:, None]
    key_block = jnp.arange(blocks, dtype=jnp.int32)[None, :]
    asking = query_block // per_dev
    holding = key_block // per_dev
    granted = subset[:, query_block[:, 0] // per_dev].reshape(KVH, blocks, blocks)
    past = key_block <= query_block
    usable = past & ((holding == asking) | (holding < asking) & granted)
    forced = (key_block == query_block) | (key_block == query_block - 1) | (key_block == 0)
    forced = forced | (query_block % per_dev == 0) & (asking >= owners // 2) & (key_block == (asking - owners // 2) * per_dev + 1)
    forced = forced | (query_block % per_dev == per_dev - 1) & (asking >= 1) & (holding == 0) & granted
    forced = forced & usable
    tier = jnp.where(forced, 3, jnp.where(usable, 2, jnp.where(past, 0, 1)))
    noise = jax.random.randint(second, (KVH, blocks, blocks), 0, 4096) // (1 + holding)
    score = tier * (1 << 24) + noise * blocks + key_block
    return lax.top_k(score, NSEL)[1].astype(jnp.int32)


def block_scale(stream_key, extent, cuts, low, high):
    level, own = 1.0, jax.random.fold_in(stream_key, 6)
    for position, shards_of in cuts:
        draws = jnp.exp(jax.random.uniform(jax.random.fold_in(own, position), (shards_of,), jnp.float32, low / len(cuts), high / len(cuts)))
        level = level * jnp.repeat(draws, extent[position] // shards_of).reshape([-1 if axis == position else 1 for axis in range(len(extent))])
    return level


def bell_draw(rng, shape, spread, limit, pieces=(), kind=jnp.bfloat16):
    factor_of = block_scale(rng, shape, pieces, -0.22, 0.18) if pieces else 1.0
    array = jax.random.normal(rng, shape, jnp.float32) * spread * factor_of
    return jnp.minimum(jnp.maximum(array, -limit), limit).astype(kind)


def setup_inputs(seed: int = 0) -> dict:
    seeds = jax.random.split(jax.random.key(seed), 14)
    tokens = draw_tokens(jax.random.fold_in(seeds[13], 71), 0)
    query_weight = bell_draw(seeds[1], (D, H * HD), (D * 4 // 9) ** -0.5, 0.1875, ((1, 4),))
    chosen_key_weight = bell_draw(seeds[2], (D, KVH * HD), D ** -0.5, 0.125, ((1, 4),))
    chosen_value_weight = bell_draw(seeds[3], (D, KVH * HD), D ** -0.5, 0.125, ((1, 4),))
    summary_key_weight = bell_draw(seeds[4], (D, KVH * HD), D ** -0.5, 0.125, ((1, 4),))
    summary_value_weight = bell_draw(seeds[5], (D, KVH * HD), D ** -0.5, 0.125, ((1, 4),))
    squeeze_key_in = bell_draw(seeds[6], (CMP_LEN * HD, CMP_HIDDEN), (CMP_LEN * HD) ** -0.5, 0.125)
    squeeze_key_out = bell_draw(seeds[7], (CMP_HIDDEN, HD), (CMP_HIDDEN // 4) ** -0.5, 1.0)
    squeeze_value_in = bell_draw(seeds[8], (CMP_LEN * HD, CMP_HIDDEN), (CMP_LEN * HD) ** -0.5, 0.125)
    squeeze_value_out = bell_draw(seeds[9], (CMP_HIDDEN, HD), (CMP_HIDDEN // 16) ** -0.5, 2.0)
    gate_weight = bell_draw(seeds[10], (2, D, H), D ** -0.5, 0.125, ((2, 4),))
    output_weight = bell_draw(seeds[11], (H * HD, D), (H * HD // 64) ** -0.5, 1.0, ((0, 4),))
    chosen_blocks = draw_chosen_blocks(jax.random.fold_in(seeds[13], 71), 0)
    return dict(tokens=tokens, query_weight=query_weight, chosen_key_weight=chosen_key_weight, chosen_value_weight=chosen_value_weight, summary_key_weight=summary_key_weight, summary_value_weight=summary_value_weight, squeeze_key_in=squeeze_key_in, squeeze_key_out=squeeze_key_out, squeeze_value_in=squeeze_value_in, squeeze_value_out=squeeze_value_out, gate_weight=gate_weight, output_weight=output_weight, chosen_blocks=chosen_blocks)


ROTARY_BASE = 10000.0
NEGATIVE_FILL = -1e30


def rotate(values, positions):
    halfway = values.shape[-1] // 2
    inverse = ROTARY_BASE ** (-jnp.arange(halfway, dtype=jnp.float32) / halfway)
    angles = positions.astype(jnp.float32)[:, None] * inverse[None, :]
    cosine_rows = jnp.cos(angles)[:, None, :]
    sine_rows = jnp.sin(angles)[:, None, :]
    former = values[..., :halfway]
    latter = values[..., halfway:]
    return jnp.concatenate([former * cosine_rows - latter * sine_rows, latter * cosine_rows + former * sine_rows], -1)


def squeeze_windows(raw_rows, weight_in, weight_out):
    length = raw_rows.shape[0]
    head_count = raw_rows.shape[1]
    head_width = raw_rows.shape[2]
    padded = jnp.concatenate([raw_rows, jnp.zeros((CMP_STRIDE, head_count, head_width), raw_rows.dtype)], 0)
    segments = padded.reshape(length // CMP_STRIDE + 1, CMP_STRIDE, head_count, head_width)
    windows = jnp.concatenate([segments[:-1], segments[1:]], 1)
    flattened = windows.transpose(0, 2, 1, 3).reshape(-1, CMP_LEN * head_width)
    hidden = jax.nn.gelu(jnp.dot(flattened, weight_in, preferred_element_type=jnp.float32)).astype(jnp.bfloat16)
    return jnp.dot(hidden, weight_out, preferred_element_type=jnp.float32).reshape(length // CMP_STRIDE, head_count, head_width)


def widen(values):
    return lax.optimization_barrier(values.astype(jnp.bfloat16)).astype(jnp.float32)


def softmax_mix(scores, visible, values, pattern):
    largest = jnp.max(jnp.where(visible, scores, NEGATIVE_FILL), -1, keepdims=True)
    weights = jnp.where(visible, jnp.exp(scores - largest), 0.0)
    summed = jnp.sum(weights, -1)[..., None]
    return jnp.einsum(pattern, widen(weights), values) / jnp.maximum(summed, 1.0)


def reference(tokens, query_weight, chosen_key_weight, chosen_value_weight, summary_key_weight, summary_value_weight,
              squeeze_key_in, squeeze_key_out, squeeze_value_in, squeeze_value_out, gate_weight, output_weight, chosen_blocks):
    positions = jnp.arange(SEQ, dtype=jnp.int32)
    per_group = H // KVH
    queries = widen(rotate(jnp.dot(tokens, query_weight, preferred_element_type=jnp.float32).reshape(SEQ, H, HD), positions))
    queries = queries.reshape(SEQ, KVH, per_group, HD)
    chosen_keys = widen(rotate(jnp.dot(tokens, chosen_key_weight, preferred_element_type=jnp.float32).reshape(SEQ, KVH, HD), positions))
    chosen_values = widen(jnp.dot(tokens, chosen_value_weight, preferred_element_type=jnp.float32)).reshape(SEQ, KVH, HD)
    raw_keys = jnp.dot(tokens, summary_key_weight, preferred_element_type=jnp.float32).astype(jnp.bfloat16).reshape(SEQ, KVH, HD)
    raw_values = jnp.dot(tokens, summary_value_weight, preferred_element_type=jnp.float32).astype(jnp.bfloat16).reshape(SEQ, KVH, HD)
    summary_count = SEQ // CMP_STRIDE
    summary_ends = jnp.arange(summary_count, dtype=jnp.int32) * CMP_STRIDE + CMP_LEN - 1
    summary_keys = widen(rotate(squeeze_windows(raw_keys, squeeze_key_in, squeeze_key_out), summary_ends))
    summary_values = widen(squeeze_windows(raw_values, squeeze_value_in, squeeze_value_out))
    block_keys = chosen_keys.reshape(NB, BLK, KVH, HD).transpose(2, 0, 1, 3)
    block_values = chosen_values.reshape(NB, BLK, KVH, HD).transpose(2, 0, 1, 3)
    first_gates = jax.nn.sigmoid(jnp.dot(tokens, gate_weight[0], preferred_element_type=jnp.float32))
    second_gates = jax.nn.sigmoid(jnp.dot(tokens, gate_weight[1], preferred_element_type=jnp.float32))
    scaling = HD ** -0.5
    group_ids = jnp.arange(KVH, dtype=jnp.int32)[:, None]

    def one_block(block_id):
        first_row = block_id * BLK
        rows_here = first_row + jnp.arange(BLK, dtype=jnp.int32)
        block_queries = lax.dynamic_slice_in_dim(queries, first_row, BLK, 0)
        scores = jnp.einsum('qgrd,ngd->grqn', block_queries, summary_keys) * scaling
        visible = (summary_ends[None, :] <= rows_here[:, None])[None, None]
        compressed = softmax_mix(scores, visible, summary_values, 'grqn,ngd->grqd')
        listed = lax.dynamic_index_in_dim(chosen_blocks, block_id, 1, keepdims=False)
        picked_keys = block_keys[group_ids, listed]
        picked_values = block_values[group_ids, listed].reshape(KVH, NSEL * BLK, HD)
        scores = jnp.einsum('qgrd,gkld->grqkl', block_queries, picked_keys).reshape(KVH, per_group, BLK, NSEL * BLK) * scaling
        key_positions = (listed[:, :, None] * BLK + jnp.arange(BLK, dtype=jnp.int32)).reshape(KVH, NSEL * BLK)
        visible = (key_positions[:, None, :] <= rows_here[None, :, None])[:, None]
        selected = softmax_mix(scores, visible, picked_values, 'grqk,gkd->grqd')
        gate_one = lax.dynamic_slice_in_dim(first_gates, first_row, BLK, 0).reshape(BLK, KVH, per_group).transpose(1, 2, 0)[..., None]
        gate_two = lax.dynamic_slice_in_dim(second_gates, first_row, BLK, 0).reshape(BLK, KVH, per_group).transpose(1, 2, 0)[..., None]
        blended = gate_one * compressed + gate_two * selected
        return blended.transpose(2, 0, 1, 3).reshape(BLK, H * HD).astype(jnp.bfloat16)

    blended = lax.map(one_block, jnp.arange(NB, dtype=jnp.int32)).reshape(SEQ, H * HD)
    heads_per_device = H // N_TP
    grouped_rows = blended.reshape(SEQ, N_TP, heads_per_device * HD)
    grouped_weight = output_weight.reshape(N_TP, heads_per_device * HD, D)

    def add_group(summed, group_id):
        rows_part = lax.dynamic_index_in_dim(grouped_rows, group_id, 1, keepdims=False)
        weight_part = lax.dynamic_index_in_dim(grouped_weight, group_id, 0, keepdims=False)
        part_sum = widen(jnp.dot(rows_part, weight_part, preferred_element_type=jnp.float32))
        return summed + part_sum, None

    grand_total, _ = lax.scan(add_group, jnp.zeros((SEQ, D), jnp.float32), jnp.arange(N_TP, dtype=jnp.int32))
    return grand_total.astype(jnp.bfloat16)
```

```python
import functools

import numpy as np
import jax
import jax.numpy as jnp
from jax import lax
from jax.experimental import pallas as pl
from jax.experimental.pallas import tpu as pltpu
from jax.sharding import PartitionSpec as P

HD = 64
CMP_LEN = 32
CMP_STRIDE = 16
BLK = 32
CAP = 4
LANES = 128


ROTARY_BASE = 10000.0
NEGATIVE_FILL = -1e30


def from_behind(block, axis, distance):
    devices = range(lax.axis_size(axis))
    route = [(i - distance, i) for i in devices if i - distance in devices]
    return lax.ppermute(block, axis, route)


def rotate(values, positions):
    halfway = values.shape[-1] // 2
    inverse = ROTARY_BASE ** (-jnp.arange(halfway, dtype=jnp.float32) / halfway)
    angles = positions.astype(jnp.float32)[:, None] * inverse[None, :]
    cosine_rows = jnp.cos(angles)[:, None, :]
    sine_rows = jnp.sin(angles)[:, None, :]
    former = values[..., :halfway]
    latter = values[..., halfway:]
    return jnp.concatenate(
        [former * cosine_rows - latter * sine_rows, latter * cosine_rows + former * sine_rows], -1
    )


def squeeze_windows(windows, weight_in, weight_out):
    total_windows = windows.shape[0]
    groups = windows.shape[2]
    head_width = windows.shape[3]
    flattened = windows.transpose(0, 2, 1, 3).reshape(total_windows * groups, CMP_LEN * head_width)
    hidden = jax.nn.gelu(jnp.dot(flattened, weight_in, preferred_element_type=jnp.float32)).astype(
        jnp.bfloat16
    )
    return jnp.dot(hidden, weight_out, preferred_element_type=jnp.float32).reshape(
        total_windows, groups, head_width
    )


def online_step(running, scores, visible, values):
    largest, summed, weighted = running
    updated = jnp.maximum(largest, jnp.max(jnp.where(visible, scores, NEGATIVE_FILL), -1))
    weights = jnp.where(visible, jnp.exp(scores - updated[..., None]), 0.0)
    shrink = jnp.exp(largest - updated)
    summed = summed * shrink + jnp.sum(weights, -1)
    weighted = weighted * shrink[..., None] + jnp.einsum(
        "grqk,kgd->grqd", weights.astype(jnp.bfloat16), values, preferred_element_type=jnp.float32
    )
    return (updated, summed, weighted)


def on_device(
    tokens,
    query_weight,
    chosen_key_weight,
    chosen_value_weight,
    summary_key_weight,
    summary_value_weight,
    squeeze_key_in,
    squeeze_key_out,
    squeeze_value_in,
    squeeze_value_out,
    gate_weight,
    output_weight,
    chosen_blocks,
):
    tok_rows = tokens.shape[0]
    heads_here = query_weight.shape[1] // HD
    groups_here = chosen_key_weight.shape[1] // HD
    per_group = heads_here // groups_here
    kv_rank = lax.axis_index("kv")
    offset = kv_rank * tok_rows
    positions = offset + jnp.arange(tok_rows, dtype=jnp.int32)
    queries = rotate(
        jnp.dot(tokens, query_weight, preferred_element_type=jnp.float32).reshape(
            tok_rows, heads_here, HD
        ),
        positions,
    )
    queries = queries.astype(jnp.bfloat16).reshape(tok_rows, groups_here, per_group, HD)
    chosen_keys = rotate(
        jnp.dot(tokens, chosen_key_weight, preferred_element_type=jnp.float32).reshape(
            tok_rows, groups_here, HD
        ),
        positions,
    ).astype(jnp.bfloat16)
    chosen_values = (
        jnp.dot(tokens, chosen_value_weight, preferred_element_type=jnp.float32)
        .astype(jnp.bfloat16)
        .reshape(tok_rows, groups_here, HD)
    )
    chosen_pairs = jnp.concatenate([chosen_keys, chosen_values], -1)
    raw_keys = (
        jnp.dot(tokens, summary_key_weight, preferred_element_type=jnp.float32)
        .astype(jnp.bfloat16)
        .reshape(tok_rows, groups_here, HD)
    )
    raw_values = (
        jnp.dot(tokens, summary_value_weight, preferred_element_type=jnp.float32)
        .astype(jnp.bfloat16)
        .reshape(tok_rows, groups_here, HD)
    )
    raw_pairs = jnp.concatenate([raw_keys, raw_values], -1)
    following = from_behind(raw_pairs[:CMP_STRIDE], "kv", -1)
    extended = jnp.concatenate([raw_pairs, following], 0)
    summary_count = tok_rows // CMP_STRIDE
    segments = extended.reshape(summary_count + 1, CMP_STRIDE, groups_here, 2 * HD)
    windows = jnp.concatenate([segments[:-1], segments[1:]], 1)
    summary_ends = (
        (kv_rank * summary_count + jnp.arange(summary_count, dtype=jnp.int32)) * CMP_STRIDE
        + CMP_LEN
        - 1
    )
    summary_keys = rotate(
        squeeze_windows(windows[..., :HD], squeeze_key_in, squeeze_key_out), summary_ends
    ).astype(jnp.bfloat16)
    summary_values = squeeze_windows(windows[..., HD:], squeeze_value_in, squeeze_value_out).astype(
        jnp.bfloat16
    )
    summaries = jnp.concatenate([summary_keys, summary_values], -1)
    scaling = HD ** (-0.5)
    starting = (
        jnp.full((groups_here, per_group, tok_rows), NEGATIVE_FILL, jnp.float32),
        jnp.zeros((groups_here, per_group, tok_rows), jnp.float32),
        jnp.zeros((groups_here, per_group, tok_rows, HD), jnp.float32),
    )
    portion = lax.all_gather(summaries, "kv", axis=0, tiled=True)
    length = portion.shape[0]
    ends = jnp.arange(length, dtype=jnp.int32) * CMP_STRIDE + CMP_LEN - 1
    scores = (
        jnp.einsum("qgrd,kgd->grqk", queries, portion[..., :HD], preferred_element_type=jnp.float32)
        * scaling
    )
    visible = (ends[None, :] <= positions[:, None])[None, None]
    folded = online_step(starting, scores, visible, portion[..., HD:])
    compressed = folded[2] / jnp.maximum(folded[1], 1.0)[..., None]
    block_count = tok_rows // BLK

    def span_step(running, stretch, leading):
        length = stretch.shape[0]
        key_positions = leading + jnp.arange(length, dtype=jnp.int32)
        listed = jnp.any(
            chosen_blocks[:, :, :, None] == (key_positions // BLK)[None, None, None, :], axis=2
        )
        listed = jnp.broadcast_to(
            listed[:, :, None, :], (groups_here, block_count, BLK, length)
        ).reshape(groups_here, tok_rows, length)
        visible = (listed & (key_positions[None, None, :] <= positions[None, :, None]))[:, None]
        scores = (
            jnp.einsum(
                "qgrd,kgd->grqk", queries, stretch[..., :HD], preferred_element_type=jnp.float32
            )
            * scaling
        )
        return online_step(running, scores, visible, stretch[..., HD:])

    def maybe_step(running, stretch, leading):

        def step_taken(carried):
            return span_step(carried, stretch, leading)

        def step_skipped(carried):
            return carried

        return lax.cond(leading <= offset + tok_rows - 1, step_taken, step_skipped, running)

    portion = lax.all_gather(chosen_pairs, "kv", axis=0, tiled=True)
    length = portion.shape[0]
    stretch_rows = tok_rows * 4

    def visit_span(number, carried):
        stretch = lax.dynamic_slice_in_dim(portion, number * stretch_rows, stretch_rows, 0)
        return maybe_step(carried, stretch, number * stretch_rows)

    folded_chosen = lax.fori_loop(0, length // stretch_rows, visit_span, starting)
    selected = folded_chosen[2] / folded_chosen[1][..., None]
    first_gates = jax.nn.sigmoid(
        jnp.dot(tokens, gate_weight[0], preferred_element_type=jnp.float32)
    )
    second_gates = jax.nn.sigmoid(
        jnp.dot(tokens, gate_weight[1], preferred_element_type=jnp.float32)
    )
    first_gates = first_gates.reshape(tok_rows, groups_here, per_group).transpose(1, 2, 0)[
        ..., None
    ]
    second_gates = second_gates.reshape(tok_rows, groups_here, per_group).transpose(1, 2, 0)[
        ..., None
    ]
    blended = (
        (first_gates * compressed + second_gates * selected)
        .transpose(2, 0, 1, 3)
        .reshape(tok_rows, heads_here * HD)
        .astype(jnp.bfloat16)
    )
    attended = lax.psum_scatter(
        jnp.dot(blended, output_weight, preferred_element_type=jnp.float32).astype(jnp.bfloat16),
        "tp",
        scatter_dimension=0,
        tiled=True,
    )
    return attended


def dot(a, b):
    return jnp.dot(a, b, preferred_element_type=jnp.float32)


def dot_nt(a, b):
    return lax.dot_general(a, b, (((1,), (1,)), ((), ())), preferred_element_type=jnp.float32)


def low_half(shape):
    return lax.broadcasted_iota(jnp.int32, shape, 1) < HD


def turn(x, cos, sin):
    quarter = HD // 2
    lane = lax.broadcasted_iota(jnp.int32, x.shape, 1)
    swapped = jnp.where(
        lane % HD < quarter, pltpu.roll(x, LANES - quarter, 1), pltpu.roll(x, quarter, 1)
    )
    return x * cos + swapped * sin


def pair_halves(a, b):
    low = low_half(a.shape)
    return jnp.where(low, a, pltpu.roll(b, HD, 1)), jnp.where(low, pltpu.roll(a, HD, 1), b)


def layer_kernel(
    n,
    groups,
    per_group,
    loc_ref,
    tokens_hbm,
    wq_hbm,
    wck_hbm,
    wcv_hbm,
    wsk_hbm,
    wsv_hbm,
    ski_hbm,
    svi_hbm,
    sko_ref,
    svo_ref,
    gate_ref,
    wo_hbm,
    slots_ref,
    keypos_ref,
    turns_ref,
    bases_ref,
    sturns_ref,
    out_ref,
    tok,
    wq,
    wc,
    ws,
    wki,
    wvi,
    wo,
    slotbuf,
    kvc,
    kvstage,
    kvbuf,
    rawf,
    halo_out,
    halo_in,
    sumown,
    sumbuf,
    qbuf,
    gates,
    gath,
    blended,
    part_a,
    part_b,
    part_c,
    got_a,
    got_b,
    got_c,
    load_sem,
    slot_send,
    slot_recv,
    kv_send,
    kv_recv,
    sum_send,
    sum_recv,
    halo_send,
    halo_recv,
    rs_send,
    rs_recv,
):
    me = lax.axis_index("kv")
    tp = lax.axis_index("tp")
    rows = tok.shape[0]
    blocks = rows // BLK
    heads = groups * per_group
    depth = tok.shape[1]
    wide = CAP * BLK
    own_base = n * CAP
    summaries = rows // CMP_STRIDE
    half = wki.shape[0]
    partner = tp + 1 - 2 * (tp % 2)
    across = (tp + 2) % 4
    diagonal = partner + 2 - 4 * (partner // 2)

    loads = []

    def load(src, dst):
        copy = pltpu.make_async_copy(src, dst, load_sem.at[len(loads)])
        copy.start()
        loads.append(copy)
        return copy

    load_c = [
        load(tokens_hbm, tok),
        load(wck_hbm, wc.at[:, 0:LANES]),
        load(wcv_hbm, wc.at[:, LANES : 2 * LANES]),
    ]
    load_s = [
        load(wsk_hbm, ws.at[:, 0:LANES]),
        load(wsv_hbm, ws.at[:, LANES : 2 * LANES]),
    ]
    load_i = [
        load(ski_hbm.at[0:half], wki.at[:, 0:LANES]),
        load(ski_hbm.at[half : 2 * half], wki.at[:, LANES : 2 * LANES]),
        load(svi_hbm.at[0:half], wvi.at[:, 0:LANES]),
        load(svi_hbm.at[half : 2 * half], wvi.at[:, LANES : 2 * LANES]),
    ]
    load_q = [load(wq_hbm, wq)]
    load_o = [load(wo_hbm, wo)]

    sumbuf[...] = jnp.zeros_like(sumbuf)
    halo_in[...] = jnp.zeros_like(halo_in)
    halo_out[...] = jnp.zeros_like(halo_out)

    barrier = pltpu.get_barrier_semaphore()
    for d in range(1, n):
        pl.semaphore_signal(
            barrier, inc=1, device_id={"kv": (me + d) % n}, device_id_type=pl.DeviceIdType.MESH
        )
    for other in (partner, across):
        pl.semaphore_signal(
            barrier, inc=1, device_id={"tp": other}, device_id_type=pl.DeviceIdType.MESH
        )
    pl.semaphore_wait(barrier, n + 1)

    def slot_copy(d, src_rank, dst_rank):
        return pltpu.make_async_remote_copy(
            src_ref=slots_ref,
            dst_ref=slotbuf.at[src_rank],
            send_sem=slot_send.at[d],
            recv_sem=slot_recv.at[src_rank],
            device_id={"kv": dst_rank},
            device_id_type=pl.DeviceIdType.MESH,
        )

    def kv_copy(d, src_rank, dst_rank):
        return pltpu.make_async_remote_copy(
            src_ref=kvstage.at[d],
            dst_ref=kvbuf.at[:, pl.ds(src_rank * CAP, CAP)],
            send_sem=kv_send.at[d],
            recv_sem=kv_recv.at[src_rank],
            device_id={"kv": dst_rank},
            device_id_type=pl.DeviceIdType.MESH,
        )

    def sum_copy(d, src_rank, dst_rank):
        return pltpu.make_async_remote_copy(
            src_ref=sumown,
            dst_ref=sumbuf.at[:, pl.ds(src_rank * summaries, summaries), :],
            send_sem=sum_send.at[d],
            recv_sem=sum_recv.at[src_rank],
            device_id={"kv": dst_rank},
            device_id_type=pl.DeviceIdType.MESH,
        )

    def halo_copy(dst_rank):
        return pltpu.make_async_remote_copy(
            src_ref=halo_out,
            dst_ref=halo_in,
            send_sem=halo_send,
            recv_sem=halo_recv,
            device_id={"kv": dst_rank},
            device_id_type=pl.DeviceIdType.MESH,
        )

    def rs_copy(k, src, dst, target):
        return pltpu.make_async_remote_copy(
            src_ref=src,
            dst_ref=dst,
            send_sem=rs_send.at[k],
            recv_sem=rs_recv.at[k],
            device_id={"tp": target},
            device_id_type=pl.DeviceIdType.MESH,
        )

    for d in range(1, n):

        @pl.when(me - d >= 0)
        def _(d=d):
            slot_copy(d, me, me - d).start()

    base_cos = bases_ref[me, 0:1, :]
    base_sin = bases_ref[me, 1:2, :]
    sign = jnp.where(
        lax.broadcasted_iota(jnp.int32, (1, LANES), 1) % HD < HD // 2, -1.0, 1.0
    )

    def tables(first, count):
        c = turns_ref[0, first : first + count, :]
        s = turns_ref[1, first : first + count, :]
        return c * base_cos - s * base_sin, (s * base_cos + c * base_sin) * sign

    for copy in load_c:
        copy.wait()
    step = 128
    for first in range(0, rows, step):
        both = dot(tok[first : first + step, :], wc[...])
        cos, sin = tables(first, step)
        keys = turn(both[:, 0:LANES], cos, sin)
        pairs = pair_halves(keys, both[:, LANES : 2 * LANES])
        for g in range(groups):
            pair = pairs[g].astype(jnp.bfloat16)
            kvc[g, first : first + step, :] = pair
            for k in range(step // BLK):
                kvbuf[g, own_base + first // BLK + k] = pair[k * BLK : (k + 1) * BLK, :]

    j = lax.broadcasted_iota(jnp.int32, (n * blocks, rows), 0)
    c = lax.broadcasted_iota(jnp.int32, (n * blocks, rows), 1)
    expand = jnp.where(j == me * blocks + c // BLK, 1.0, 0.0).astype(jnp.bfloat16)
    row = lax.broadcasted_iota(jnp.int32, (wide, rows), 0)
    col = lax.broadcasted_iota(jnp.int32, (wide, rows), 1)
    same_place = row % BLK == col % BLK
    row_slot = (row // BLK).astype(jnp.float32)
    for d in range(n - 1, 0, -1):

        @pl.when(me + d < n)
        def _(d=d):
            slot_copy(d, me + d, me).wait_recv()
            asked = dot(slotbuf[me + d].astype(jnp.bfloat16), expand)
            for g in range(groups):
                pick = jnp.where(same_place & (asked[g : g + 1, :] == row_slot), 1.0, 0.0)
                packed = dot(pick.astype(jnp.bfloat16), kvc[g]).astype(jnp.bfloat16)
                for k in range(CAP):
                    kvstage[d, g, k] = packed[k * BLK : (k + 1) * BLK, :]
            kv_copy(d, me, me + d).start()

    for copy in load_s:
        copy.wait()
    for first in range(0, rows, step):
        both = dot(tok[first : first + step, :], ws[...])
        rounded = both.astype(jnp.bfloat16).astype(jnp.float32)
        for kind in range(2):
            rawf[kind, first : first + step, :] = rounded[:, kind * LANES : (kind + 1) * LANES]
    for copy in load_i:
        copy.wait()
    layers = []
    for kind, weight in ((0, wki), (1, wvi)):
        pieces = [[] for _ in range(groups)]
        for p in range(0, CMP_STRIDE, 2):
            one = rawf[kind, pl.ds(p, summaries, stride=CMP_STRIDE), :]
            two = rawf[kind, pl.ds(p + 1, summaries, stride=CMP_STRIDE), :]
            for g, piece in enumerate(pair_halves(one, two)):
                pieces[g].append(piece.astype(jnp.bfloat16))
        segments = jnp.concatenate([jnp.concatenate(pieces[g], 1) for g in range(groups)], 0)
        layers.append(dot(segments, weight[...]))
    for kind in range(2):
        for g in range(groups):
            at = kind * groups + g
            halo_out[at : at + 1, :] = layers[kind][
                g * summaries : g * summaries + 1, LANES : 2 * LANES
            ]

    @pl.when(me > 0)
    def _():
        halo_copy(me - 1).start()

    for copy in load_q:
        copy.wait()
    scaling = HD**-0.5
    for first in range(0, rows, step):
        projected = dot(tok[first : first + step, :], wq[...])
        cos, sin = tables(first, step)
        cos = cos * scaling
        sin = sin * scaling
        for pair in range(heads // 2):
            turned = turn(projected[:, pair * LANES : (pair + 1) * LANES], cos, sin)
            low = low_half(turned.shape)
            for odd in range(2):
                head = 2 * pair + odd
                g, r = head // per_group, head % per_group
                part = pltpu.roll(turned, HD, 1) if odd else turned
                part = jnp.where(low, part, 0.0).astype(jnp.bfloat16)
                for k in range(step // BLK):
                    at = (first // BLK + k) * per_group * BLK + r * BLK
                    qbuf[g, at : at + BLK, :] = part[k * BLK : (k + 1) * BLK, :]
    gates[...] = jax.nn.sigmoid(dot_nt(tok[...], gate_ref[...]))

    @pl.when(me < n - 1)
    def _():
        halo_copy(me).wait_recv()

    hidden = []
    last = lax.broadcasted_iota(jnp.int32, (summaries, LANES), 0) == summaries - 1
    for kind in range(2):
        per = []
        for g in range(groups):
            here = layers[kind][g * summaries : (g + 1) * summaries, :]
            at = kind * groups + g
            following = jnp.where(
                last, halo_in[at : at + 1, :], pltpu.roll(here[:, LANES:], summaries - 1, 0)
            )
            per.append(here[:, :LANES] + following)
        hidden.append(jax.nn.gelu(jnp.concatenate(per, 0)).astype(jnp.bfloat16))
    summed = dot(hidden[0], sko_ref[...]) + dot(hidden[1], svo_ref[...])
    low = low_half((summaries, LANES))
    sc = sturns_ref[0]
    ss = sturns_ref[1]
    scos = jnp.where(low, sc * base_cos - ss * base_sin, 1.0)
    ssin = jnp.where(low, (ss * base_cos + sc * base_sin) * sign, 0.0)
    for g in range(groups):
        pair = turn(summed[g * summaries : (g + 1) * summaries, :], scos, ssin)
        pair = pair.astype(jnp.bfloat16)
        sumown[g] = pair
        sumbuf[g, pl.ds(pl.multiple_of(me * summaries, summaries), summaries), :] = pair
    for d in range(1, n):

        @pl.when(me + d < n)
        def _(d=d):
            sum_copy(d, me, me + d).start()

    for d in range(1, n):

        @pl.when(me - d >= 0)
        def _(d=d):
            sum_copy(d, me - d, me).wait_recv()
            kv_copy(d, me - d, me).wait_recv()

    total = n * summaries
    listed = keypos_ref.shape[1]
    qrows = per_group * BLK
    in_block = lax.broadcasted_iota(jnp.int32, (qrows, 1), 0) % BLK
    ends = lax.broadcasted_iota(jnp.int32, (1, total), 1) * CMP_STRIDE + CMP_LEN - 1
    per_chunk = blocks // 4

    def mix(q, pairs, visible):
        scores = jnp.where(visible, dot_nt(q, pairs), NEGATIVE_FILL)
        largest = jnp.max(scores, -1, keepdims=True)
        weights = jnp.where(visible, jnp.exp(scores - largest), 0.0)
        total_weight = jnp.sum(weights, -1, keepdims=True)
        return dot(weights.astype(jnp.bfloat16), pairs), total_weight

    def attend(target):
        def block(i, _):
            b = target * per_chunk + i
            pos = me * rows + b * BLK + in_block
            gate = gates[pl.ds(pl.multiple_of(b * BLK, BLK), BLK), :]
            for g in range(groups):
                q = qbuf[g, pl.ds(pl.multiple_of(b * qrows, qrows), qrows), :]
                for k in range(listed // BLK):
                    where = loc_ref[g * blocks + b, k]
                    gath[g, k * BLK : (k + 1) * BLK, :] = kvbuf[g, where]
                compressed, csum = mix(q, sumbuf[g], ends <= pos)
                key_positions = keypos_ref[pl.ds(g * blocks + b, 1), :]
                selected, ssum = mix(q, gath[g], key_positions <= pos)
                cinv = 1.0 / jnp.maximum(csum, 1.0)
                sinv = 1.0 / ssum
                heads_out = []
                for r in range(per_group):
                    part = slice(r * BLK, (r + 1) * BLK)
                    h = g * per_group + r
                    heads_out.append(
                        compressed[part] * (cinv[part] * gate[:, h : h + 1])
                        + selected[part] * (sinv[part] * gate[:, heads + h : heads + h + 1])
                    )
                for r in range(0, per_group, 2):
                    joined = jnp.where(
                        low_half((BLK, LANES)), pltpu.roll(heads_out[r], HD, 1), heads_out[r + 1]
                    )
                    at = (g * per_group + r) * HD
                    blended[pl.ds(pl.multiple_of(i * BLK, BLK), BLK), at : at + LANES] = (
                        joined.astype(jnp.bfloat16)
                    )
            return 0

        lax.fori_loop(0, per_chunk, block, 0)

    tile = 512
    columns = wo.shape[1]

    def project(dst, added):
        for at in range(0, columns, tile):
            piece = dot(blended[...], wo[:, at : at + tile])
            for other in added:
                piece = piece + other[:, at : at + tile].astype(jnp.float32)
            dst[:, at : at + tile] = piece.astype(jnp.bfloat16)

    attend(diagonal)
    for copy in load_o:
        copy.wait()
    project(part_a, [])
    send_a = rs_copy(0, part_a, got_a, partner)
    send_a.start()
    attend(across)
    send_a.wait_recv()
    project(part_b, [got_a])
    send_b = rs_copy(1, part_b, got_b, across)
    send_b.start()
    attend(partner)
    project(part_c, [])
    send_c = rs_copy(2, part_c, got_c, partner)
    send_c.start()
    attend(tp)
    send_c.wait_recv()
    send_b.wait_recv()
    project(out_ref, [got_c, got_b])

    for copy in (send_a, send_b, send_c):
        copy.wait_send()
    for d in range(1, n):

        @pl.when(me - d >= 0)
        def _(d=d):
            slot_copy(d, me, me - d).wait_send()

        @pl.when(me + d < n)
        def _(d=d):
            kv_copy(d, me, me + d).wait_send()
            sum_copy(d, me, me + d).wait_send()

    @pl.when(me > 0)
    def _():
        halo_copy(me - 1).wait_send()


def rotary_constants(rows, n):
    inverse = ROTARY_BASE ** (-np.arange(HD // 2) / (HD // 2))
    lanes = np.tile(inverse, LANES // (HD // 2))[None, :]

    def table(positions):
        angles = np.asarray(positions, np.float64)[:, None] * lanes
        return np.stack([np.cos(angles), np.sin(angles)]).astype(np.float32)

    local = table(np.arange(rows))
    bases = table(np.arange(n) * rows).transpose(1, 0, 2)
    ends = table(np.arange(rows // CMP_STRIDE) * CMP_STRIDE + CMP_LEN - 1)
    return local, bases, ends


def fused(n, *args):
    (
        tokens,
        wq,
        wck,
        wcv,
        wsk,
        wsv,
        ski,
        sko,
        svi,
        svo,
        gate_weight,
        wo,
        chosen,
    ) = args
    rows, depth = tokens.shape
    groups = wck.shape[1] // HD
    per_group = wq.shape[1] // wck.shape[1]
    heads = groups * per_group
    blocks = rows // BLK
    listed = chosen.shape[2]
    me = lax.axis_index("kv")
    query_block = me * blocks + jnp.arange(blocks, dtype=jnp.int32)
    every = n * blocks
    hit = chosen[..., None] == jnp.arange(every, dtype=jnp.int32)
    counted = hit & (chosen <= query_block[None, :, None])[..., None]
    present = jnp.any(counted, axis=(1, 2))
    by_shard = present.reshape(groups, n, blocks).astype(jnp.int32)
    earlier = jnp.arange(blocks)[:, None] < jnp.arange(blocks)[None, :]
    slot = jnp.sum(jnp.where(earlier, by_shard[..., None], 0), axis=2).reshape(groups, every)
    slots = jnp.where(present, slot, -1).astype(jnp.float32)
    slots = jnp.pad(slots, ((0, 8 - groups), (0, 0)), constant_values=-1.0)
    chosen_slot = jnp.sum(jnp.where(hit, slot[:, None, None, :], 0), -1)
    owner = chosen // blocks
    loc = jnp.where(
        owner == me,
        n * CAP + chosen % blocks,
        jnp.where(owner < me, owner * CAP + jnp.minimum(chosen_slot, CAP - 1), n * CAP),
    ).reshape(groups * blocks, listed)
    keypos = (
        chosen[..., None] * BLK + jnp.arange(BLK, dtype=jnp.int32)
    ).reshape(groups * blocks, listed * BLK)
    gate = gate_weight.transpose(0, 2, 1).reshape(2 * heads, depth)
    gate = jnp.pad(gate, ((0, LANES - 2 * heads), (0, 0)))
    sko = jnp.pad(sko, ((0, 0), (0, HD)))
    svo = jnp.pad(svo, ((0, 0), (HD, 0)))
    local, bases, ends = rotary_constants(rows, n)
    chunk = rows // 4
    bf = jnp.bfloat16
    hbm = pl.BlockSpec(memory_space=pl.ANY)
    vmem = pl.BlockSpec(memory_space=pltpu.VMEM)
    wide = CAP * BLK
    summaries = rows // CMP_STRIDE
    part = pltpu.VMEM((chunk, wo.shape[1]), bf)
    dma = pltpu.SemaphoreType.DMA
    return pl.pallas_call(
        functools.partial(layer_kernel, n, groups, per_group),
        out_shape=jax.ShapeDtypeStruct((chunk, wo.shape[1]), bf),
        in_specs=[pl.BlockSpec(memory_space=pltpu.SMEM)]
        + [hbm] * 8
        + [vmem] * 3
        + [hbm]
        + [vmem] * 5,
        out_specs=vmem,
        scratch_shapes=[
            pltpu.VMEM((rows, depth), bf),
            pltpu.VMEM((depth, heads * HD), bf),
            pltpu.VMEM((depth, 2 * LANES), bf),
            pltpu.VMEM((depth, 2 * LANES), bf),
            pltpu.VMEM((CMP_STRIDE * HD, 2 * LANES), bf),
            pltpu.VMEM((CMP_STRIDE * HD, 2 * LANES), bf),
            pltpu.VMEM(wo.shape, bf),
            pltpu.VMEM((n, 8, every), jnp.float32),
            pltpu.VMEM((groups, rows, LANES), bf),
            pltpu.VMEM((n, groups, CAP, BLK, LANES), bf),
            pltpu.VMEM((groups, n * CAP + blocks, BLK, LANES), bf),
            pltpu.VMEM((2, rows, LANES), jnp.float32),
            pltpu.VMEM((8, LANES), jnp.float32),
            pltpu.VMEM((8, LANES), jnp.float32),
            pltpu.VMEM((groups, summaries, LANES), bf),
            pltpu.VMEM((groups, n * summaries, LANES), bf),
            pltpu.VMEM((groups, rows * per_group, LANES), bf),
            pltpu.VMEM((rows, LANES), jnp.float32),
            pltpu.VMEM((groups, listed * BLK, LANES), bf),
            pltpu.VMEM((chunk, heads * HD), bf),
            part,
            part,
            part,
            part,
            part,
            part,
            dma((11,)),
            dma((n,)),
            dma((n,)),
            dma((n,)),
            dma((n,)),
            dma((n,)),
            dma((n,)),
            dma(()),
            dma(()),
            dma((3,)),
            dma((3,)),
        ],
        compiler_params=pltpu.CompilerParams(
            collective_id=0, has_side_effects=True, vmem_limit_bytes=60 * 1024 * 1024
        ),
        name="layer",
    )(loc, tokens, wq, wck, wcv, wsk, wsv, ski, svi, sko, svo, gate, wo, slots, keypos, local, bases, ends)


def solution(mesh):
    n = mesh.shape["kv"]

    def one_device(*args):
        fits = args[2].shape[1] == LANES and mesh.shape["tp"] == 4
        return fused(n, *args) if fits else on_device(*args)

    return jax.shard_map(
        one_device,
        mesh=mesh,
        in_specs=(
            P("kv", None),
            P(None, "tp"),
            P(None, "tp"),
            P(None, "tp"),
            P(None, "tp"),
            P(None, "tp"),
            P(),
            P(),
            P(),
            P(),
            P(None, None, "tp"),
            P("tp", None),
            P("tp", "kv", None),
        ),
        out_specs=P(("kv", "tp"), None),
        check_vma=False,
    )
```

```python
import functools

import numpy as np
import jax
import jax.numpy as jnp
from jax import lax
from jax.experimental import pallas as pl
from jax.experimental.pallas import tpu as pltpu
from jax.sharding import PartitionSpec as P

HD = 64
CMP_LEN = 32
CMP_STRIDE = 16
BLK = 32
CAP = 4
LANES = 128


ROTARY_BASE = 10000.0
NEGATIVE_FILL = -1e30


def from_behind(block, axis, distance):
    devices = range(lax.axis_size(axis))
    route = [(i - distance, i) for i in devices if i - distance in devices]
    return lax.ppermute(block, axis, route)


def rotate(values, positions):
    halfway = values.shape[-1] // 2
    inverse = ROTARY_BASE ** (-jnp.arange(halfway, dtype=jnp.float32) / halfway)
    angles = positions.astype(jnp.float32)[:, None] * inverse[None, :]
    cosine_rows = jnp.cos(angles)[:, None, :]
    sine_rows = jnp.sin(angles)[:, None, :]
    former = values[..., :halfway]
    latter = values[..., halfway:]
    return jnp.concatenate(
        [former * cosine_rows - latter * sine_rows, latter * cosine_rows + former * sine_rows], -1
    )


def squeeze_windows(windows, weight_in, weight_out):
    total_windows = windows.shape[0]
    groups = windows.shape[2]
    head_width = windows.shape[3]
    flattened = windows.transpose(0, 2, 1, 3).reshape(total_windows * groups, CMP_LEN * head_width)
    hidden = jax.nn.gelu(jnp.dot(flattened, weight_in, preferred_element_type=jnp.float32)).astype(
        jnp.bfloat16
    )
    return jnp.dot(hidden, weight_out, preferred_element_type=jnp.float32).reshape(
        total_windows, groups, head_width
    )


def online_step(running, scores, visible, values):
    largest, summed, weighted = running
    updated = jnp.maximum(largest, jnp.max(jnp.where(visible, scores, NEGATIVE_FILL), -1))
    weights = jnp.where(visible, jnp.exp(scores - updated[..., None]), 0.0)
    shrink = jnp.exp(largest - updated)
    summed = summed * shrink + jnp.sum(weights, -1)
    weighted = weighted * shrink[..., None] + jnp.einsum(
        "grqk,kgd->grqd", weights.astype(jnp.bfloat16), values, preferred_element_type=jnp.float32
    )
    return (updated, summed, weighted)


def on_device(
    tokens,
    query_weight,
    chosen_key_weight,
    chosen_value_weight,
    summary_key_weight,
    summary_value_weight,
    squeeze_key_in,
    squeeze_key_out,
    squeeze_value_in,
    squeeze_value_out,
    gate_weight,
    output_weight,
    chosen_blocks,
):
    tok_rows = tokens.shape[0]
    heads_here = query_weight.shape[1] // HD
    groups_here = chosen_key_weight.shape[1] // HD
    per_group = heads_here // groups_here
    kv_rank = lax.axis_index("kv")
    offset = kv_rank * tok_rows
    positions = offset + jnp.arange(tok_rows, dtype=jnp.int32)
    queries = rotate(
        jnp.dot(tokens, query_weight, preferred_element_type=jnp.float32).reshape(
            tok_rows, heads_here, HD
        ),
        positions,
    )
    queries = queries.astype(jnp.bfloat16).reshape(tok_rows, groups_here, per_group, HD)
    chosen_keys = rotate(
        jnp.dot(tokens, chosen_key_weight, preferred_element_type=jnp.float32).reshape(
            tok_rows, groups_here, HD
        ),
        positions,
    ).astype(jnp.bfloat16)
    chosen_values = (
        jnp.dot(tokens, chosen_value_weight, preferred_element_type=jnp.float32)
        .astype(jnp.bfloat16)
        .reshape(tok_rows, groups_here, HD)
    )
    chosen_pairs = jnp.concatenate([chosen_keys, chosen_values], -1)
    raw_keys = (
        jnp.dot(tokens, summary_key_weight, preferred_element_type=jnp.float32)
        .astype(jnp.bfloat16)
        .reshape(tok_rows, groups_here, HD)
    )
    raw_values = (
        jnp.dot(tokens, summary_value_weight, preferred_element_type=jnp.float32)
        .astype(jnp.bfloat16)
        .reshape(tok_rows, groups_here, HD)
    )
    raw_pairs = jnp.concatenate([raw_keys, raw_values], -1)
    following = from_behind(raw_pairs[:CMP_STRIDE], "kv", -1)
    extended = jnp.concatenate([raw_pairs, following], 0)
    summary_count = tok_rows // CMP_STRIDE
    segments = extended.reshape(summary_count + 1, CMP_STRIDE, groups_here, 2 * HD)
    windows = jnp.concatenate([segments[:-1], segments[1:]], 1)
    summary_ends = (
        (kv_rank * summary_count + jnp.arange(summary_count, dtype=jnp.int32)) * CMP_STRIDE
        + CMP_LEN
        - 1
    )
    summary_keys = rotate(
        squeeze_windows(windows[..., :HD], squeeze_key_in, squeeze_key_out), summary_ends
    ).astype(jnp.bfloat16)
    summary_values = squeeze_windows(windows[..., HD:], squeeze_value_in, squeeze_value_out).astype(
        jnp.bfloat16
    )
    summaries = jnp.concatenate([summary_keys, summary_values], -1)
    scaling = HD ** (-0.5)
    starting = (
        jnp.full((groups_here, per_group, tok_rows), NEGATIVE_FILL, jnp.float32),
        jnp.zeros((groups_here, per_group, tok_rows), jnp.float32),
        jnp.zeros((groups_here, per_group, tok_rows, HD), jnp.float32),
    )
    portion = lax.all_gather(summaries, "kv", axis=0, tiled=True)
    length = portion.shape[0]
    ends = jnp.arange(length, dtype=jnp.int32) * CMP_STRIDE + CMP_LEN - 1
    scores = (
        jnp.einsum("qgrd,kgd->grqk", queries, portion[..., :HD], preferred_element_type=jnp.float32)
        * scaling
    )
    visible = (ends[None, :] <= positions[:, None])[None, None]
    folded = online_step(starting, scores, visible, portion[..., HD:])
    compressed = folded[2] / jnp.maximum(folded[1], 1.0)[..., None]
    block_count = tok_rows // BLK

    def span_step(running, stretch, leading):
        length = stretch.shape[0]
        key_positions = leading + jnp.arange(length, dtype=jnp.int32)
        listed = jnp.any(
            chosen_blocks[:, :, :, None] == (key_positions // BLK)[None, None, None, :], axis=2
        )
        listed = jnp.broadcast_to(
            listed[:, :, None, :], (groups_here, block_count, BLK, length)
        ).reshape(groups_here, tok_rows, length)
        visible = (listed & (key_positions[None, None, :] <= positions[None, :, None]))[:, None]
        scores = (
            jnp.einsum(
                "qgrd,kgd->grqk", queries, stretch[..., :HD], preferred_element_type=jnp.float32
            )
            * scaling
        )
        return online_step(running, scores, visible, stretch[..., HD:])

    def maybe_step(running, stretch, leading):

        def step_taken(carried):
            return span_step(carried, stretch, leading)

        def step_skipped(carried):
            return carried

        return lax.cond(leading <= offset + tok_rows - 1, step_taken, step_skipped, running)

    portion = lax.all_gather(chosen_pairs, "kv", axis=0, tiled=True)
    length = portion.shape[0]
    stretch_rows = tok_rows * 4

    def visit_span(number, carried):
        stretch = lax.dynamic_slice_in_dim(portion, number * stretch_rows, stretch_rows, 0)
        return maybe_step(carried, stretch, number * stretch_rows)

    folded_chosen = lax.fori_loop(0, length // stretch_rows, visit_span, starting)
    selected = folded_chosen[2] / folded_chosen[1][..., None]
    first_gates = jax.nn.sigmoid(
        jnp.dot(tokens, gate_weight[0], preferred_element_type=jnp.float32)
    )
    second_gates = jax.nn.sigmoid(
        jnp.dot(tokens, gate_weight[1], preferred_element_type=jnp.float32)
    )
    first_gates = first_gates.reshape(tok_rows, groups_here, per_group).transpose(1, 2, 0)[
        ..., None
    ]
    second_gates = second_gates.reshape(tok_rows, groups_here, per_group).transpose(1, 2, 0)[
        ..., None
    ]
    blended = (
        (first_gates * compressed + second_gates * selected)
        .transpose(2, 0, 1, 3)
        .reshape(tok_rows, heads_here * HD)
        .astype(jnp.bfloat16)
    )
    attended = lax.psum_scatter(
        jnp.dot(blended, output_weight, preferred_element_type=jnp.float32).astype(jnp.bfloat16),
        "tp",
        scatter_dimension=0,
        tiled=True,
    )
    return attended


def dot(a, b):
    return jnp.dot(a, b, preferred_element_type=jnp.float32)


def dot_nt(a, b):
    return lax.dot_general(a, b, (((1,), (1,)), ((), ())), preferred_element_type=jnp.float32)


def low_half(shape):
    return lax.broadcasted_iota(jnp.int32, shape, 1) < HD


def turn(x, cos, sin):
    quarter = HD // 2
    lane = lax.broadcasted_iota(jnp.int32, x.shape, 1)
    swapped = jnp.where(
        lane % HD < quarter, pltpu.roll(x, LANES - quarter, 1), pltpu.roll(x, quarter, 1)
    )
    return x * cos + swapped * sin


def pair_halves(a, b):
    low = low_half(a.shape)
    return jnp.where(low, a, pltpu.roll(b, HD, 1)), jnp.where(low, pltpu.roll(a, HD, 1), b)


def layer_kernel(
    n,
    groups,
    per_group,
    chosen_ref,
    chosen_vec,
    tokens_hbm,
    wq_hbm,
    wck_hbm,
    wcv_hbm,
    wsk_hbm,
    wsv_hbm,
    ski_hbm,
    svi_hbm,
    sko_ref,
    svo_ref,
    gate_ref,
    wo_hbm,
    turns_ref,
    bases_ref,
    sturns_ref,
    out_ref,
    tok,
    wq,
    wc,
    ws,
    wki,
    wvi,
    wo,
    wo_other,
    slots_ref,
    locs,
    locmap,
    slotbuf,
    kvc,
    kvstage,
    kvbuf,
    rawf,
    halo_out,
    halo_in,
    sumown,
    sumbuf,
    qbuf,
    gates,
    gath,
    compr,
    blended,
    blended_got,
    part_b,
    got_b,
    load_sem,
    slot_send,
    slot_recv,
    kv_send,
    kv_recv,
    sum_send,
    sum_recv,
    halo_send,
    halo_recv,
    rs_send,
    rs_recv,
    loc_sem,
):
    me = lax.axis_index("kv")
    tp = lax.axis_index("tp")
    rows = tok.shape[0]
    blocks = rows // BLK
    heads = groups * per_group
    depth = tok.shape[1]
    wide = CAP * BLK
    own_base = n * CAP
    summaries = rows // CMP_STRIDE
    half = wki.shape[0]
    partner = tp + 1 - 2 * (tp % 2)
    across = (tp + 2) % 4
    diagonal = partner + 2 - 4 * (partner // 2)

    loads = []

    def load(src, dst):
        copy = pltpu.make_async_copy(src, dst, load_sem.at[len(loads)])
        copy.start()
        loads.append(copy)
        return copy

    load_c = [
        load(tokens_hbm, tok),
        load(wck_hbm, wc.at[:, 0:LANES]),
        load(wcv_hbm, wc.at[:, LANES : 2 * LANES]),
    ]
    load_s = [
        load(wsk_hbm, ws.at[:, 0:LANES]),
        load(wsv_hbm, ws.at[:, LANES : 2 * LANES]),
    ]
    load_i = [
        load(ski_hbm.at[0:half], wki.at[:, 0:LANES]),
        load(ski_hbm.at[half : 2 * half], wki.at[:, LANES : 2 * LANES]),
        load(svi_hbm.at[0:half], wvi.at[:, 0:LANES]),
        load(svi_hbm.at[half : 2 * half], wvi.at[:, LANES : 2 * LANES]),
    ]

    every = n * blocks
    lane = lax.broadcasted_iota(jnp.int32, (blocks, every), 1)
    query_block = me * blocks + lax.broadcasted_iota(jnp.int32, (blocks, 1), 0)
    row8 = lax.broadcasted_iota(jnp.int32, (8, every), 0)
    lane8 = lax.broadcasted_iota(jnp.int32, (8, every), 1)
    present = jnp.zeros((8, every), jnp.int32)
    for g in range(groups):
        asked = chosen_vec[g]
        asked = jnp.where(asked <= query_block, asked, -1)
        hit = jnp.where(asked[:, 0:1] == lane, 1, 0)
        for k in range(1, asked.shape[1]):
            hit = jnp.where(asked[:, k : k + 1] == lane, 1, hit)
        hit = jnp.max(hit, 0, keepdims=True)
        present = jnp.where(row8 == g, hit, present)
    slot = jnp.zeros((8, every), jnp.int32)
    for s in range(1, blocks):
        slot = slot + jnp.where(lane8 % blocks >= s, pltpu.roll(present, s, 1), 0)
    slots_ref[...] = jnp.where(present > 0, slot, -1).astype(jnp.float32)
    owner = lane8 // blocks
    locs[...] = jnp.where(
        owner == me,
        n * CAP + lane8 % blocks,
        jnp.where(owner < me, owner * CAP + jnp.minimum(slot, CAP - 1), n * CAP),
    )

    sumbuf[...] = jnp.zeros_like(sumbuf)
    halo_in[...] = jnp.zeros_like(halo_in)
    halo_out[...] = jnp.zeros_like(halo_out)

    barrier = pltpu.get_barrier_semaphore()
    for d in range(1, n):
        pl.semaphore_signal(
            barrier, inc=1, device_id={"kv": (me + d) % n}, device_id_type=pl.DeviceIdType.MESH
        )
    for other in (partner, across):
        pl.semaphore_signal(
            barrier, inc=1, device_id={"tp": other}, device_id_type=pl.DeviceIdType.MESH
        )
    pl.semaphore_wait(barrier, n + 1)

    loc_copy = pltpu.make_async_copy(locs, locmap, loc_sem)
    loc_copy.start()

    def slot_copy(d, src_rank, dst_rank):
        return pltpu.make_async_remote_copy(
            src_ref=slots_ref,
            dst_ref=slotbuf.at[src_rank],
            send_sem=slot_send.at[d],
            recv_sem=slot_recv.at[src_rank],
            device_id={"kv": dst_rank},
            device_id_type=pl.DeviceIdType.MESH,
        )

    def kv_copy(d, src_rank, dst_rank):
        return pltpu.make_async_remote_copy(
            src_ref=kvstage.at[d],
            dst_ref=kvbuf.at[:, pl.ds(src_rank * CAP, CAP)],
            send_sem=kv_send.at[d],
            recv_sem=kv_recv.at[src_rank],
            device_id={"kv": dst_rank},
            device_id_type=pl.DeviceIdType.MESH,
        )

    def sum_copy(d, src_rank, dst_rank):
        return pltpu.make_async_remote_copy(
            src_ref=sumown,
            dst_ref=sumbuf.at[:, pl.ds(src_rank * summaries, summaries), :],
            send_sem=sum_send.at[d],
            recv_sem=sum_recv.at[src_rank],
            device_id={"kv": dst_rank},
            device_id_type=pl.DeviceIdType.MESH,
        )

    def halo_copy(dst_rank):
        return pltpu.make_async_remote_copy(
            src_ref=halo_out,
            dst_ref=halo_in,
            send_sem=halo_send,
            recv_sem=halo_recv,
            device_id={"kv": dst_rank},
            device_id_type=pl.DeviceIdType.MESH,
        )

    def rs_copy(k, src, dst, target):
        return pltpu.make_async_remote_copy(
            src_ref=src,
            dst_ref=dst,
            send_sem=rs_send.at[k],
            recv_sem=rs_recv.at[k],
            device_id={"tp": target},
            device_id_type=pl.DeviceIdType.MESH,
        )

    for d in range(1, n):

        @pl.when(me - d >= 0)
        def _(d=d):
            slot_copy(d, me, me - d).start()

    load_q = [load(wq_hbm, wq)]
    load_o = [load(wo_hbm, wo)]
    weight_copy = rs_copy(0, wo_hbm, wo_other, partner)
    weight_copy.start()

    base_cos = bases_ref[me, 0:1, :]
    base_sin = bases_ref[me, 1:2, :]
    sign = jnp.where(
        lax.broadcasted_iota(jnp.int32, (1, LANES), 1) % HD < HD // 2, -1.0, 1.0
    )

    def tables(first, count):
        c = turns_ref[0, first : first + count, :]
        s = turns_ref[1, first : first + count, :]
        return c * base_cos - s * base_sin, (s * base_cos + c * base_sin) * sign

    for copy in load_c:
        copy.wait()
    step = 128
    for first in range(0, rows, step):
        both = dot(tok[first : first + step, :], wc[...])
        cos, sin = tables(first, step)
        keys = turn(both[:, 0:LANES], cos, sin)
        pairs = pair_halves(keys, both[:, LANES : 2 * LANES])
        for g in range(groups):
            pair = pairs[g].astype(jnp.bfloat16)
            kvc[g, first : first + step, :] = pair
            for k in range(step // BLK):
                kvbuf[g, own_base + first // BLK + k] = pair[k * BLK : (k + 1) * BLK, :]

    j = lax.broadcasted_iota(jnp.int32, (n * blocks, rows), 0)
    c = lax.broadcasted_iota(jnp.int32, (n * blocks, rows), 1)
    expand = jnp.where(j == me * blocks + c // BLK, 1.0, 0.0).astype(jnp.bfloat16)
    row = lax.broadcasted_iota(jnp.int32, (wide, rows), 0)
    col = lax.broadcasted_iota(jnp.int32, (wide, rows), 1)
    same_place = row % BLK == col % BLK
    row_slot = (row // BLK).astype(jnp.float32)
    for d in range(n - 1, 0, -1):

        @pl.when(me + d < n)
        def _(d=d):
            slot_copy(d, me + d, me).wait_recv()
            asked = dot(slotbuf[me + d].astype(jnp.bfloat16), expand)
            for g in range(groups):
                pick = jnp.where(same_place & (asked[g : g + 1, :] == row_slot), 1.0, 0.0)
                packed = dot(pick.astype(jnp.bfloat16), kvc[g]).astype(jnp.bfloat16)
                for k in range(CAP):
                    kvstage[d, g, k] = packed[k * BLK : (k + 1) * BLK, :]
            kv_copy(d, me, me + d).start()

    for copy in load_s:
        copy.wait()
    for first in range(0, rows, step):
        both = dot(tok[first : first + step, :], ws[...])
        rounded = both.astype(jnp.bfloat16).astype(jnp.float32)
        for kind in range(2):
            rawf[kind, first : first + step, :] = rounded[:, kind * LANES : (kind + 1) * LANES]
    for copy in load_i:
        copy.wait()
    layers = []
    for kind, weight in ((0, wki), (1, wvi)):
        pieces = [[] for _ in range(groups)]
        for p in range(0, CMP_STRIDE, 2):
            one = rawf[kind, pl.ds(p, summaries, stride=CMP_STRIDE), :]
            two = rawf[kind, pl.ds(p + 1, summaries, stride=CMP_STRIDE), :]
            for g, piece in enumerate(pair_halves(one, two)):
                pieces[g].append(piece.astype(jnp.bfloat16))
        segments = jnp.concatenate([jnp.concatenate(pieces[g], 1) for g in range(groups)], 0)
        layers.append(dot(segments, weight[...]))
    for kind in range(2):
        for g in range(groups):
            at = kind * groups + g
            halo_out[at : at + 1, :] = layers[kind][
                g * summaries : g * summaries + 1, LANES : 2 * LANES
            ]

    @pl.when(me > 0)
    def _():
        halo_copy(me - 1).start()

    for copy in load_q:
        copy.wait()
    scaling = HD**-0.5
    for first in range(0, rows, step):
        projected = dot(tok[first : first + step, :], wq[...])
        cos, sin = tables(first, step)
        cos = cos * scaling
        sin = sin * scaling
        for pair in range(heads // 2):
            turned = turn(projected[:, pair * LANES : (pair + 1) * LANES], cos, sin)
            low = low_half(turned.shape)
            for odd in range(2):
                head = 2 * pair + odd
                g, r = head // per_group, head % per_group
                part = pltpu.roll(turned, HD, 1) if odd else turned
                part = jnp.where(low, part, 0.0).astype(jnp.bfloat16)
                for k in range(step // BLK):
                    at = (first // BLK + k) * per_group * BLK + r * BLK
                    qbuf[g, at : at + BLK, :] = part[k * BLK : (k + 1) * BLK, :]
    gate_rows = jnp.concatenate([gate_ref[k].astype(jnp.float32) for k in range(2)], 0)
    gates[...] = jax.nn.sigmoid(dot_nt(tok[...], gate_rows.astype(jnp.bfloat16)))

    @pl.when(me < n - 1)
    def _():
        halo_copy(me).wait_recv()

    hidden = []
    last = lax.broadcasted_iota(jnp.int32, (summaries, LANES), 0) == summaries - 1
    for kind in range(2):
        per = []
        for g in range(groups):
            here = layers[kind][g * summaries : (g + 1) * summaries, :]
            at = kind * groups + g
            following = jnp.where(
                last, halo_in[at : at + 1, :], pltpu.roll(here[:, LANES:], summaries - 1, 0)
            )
            per.append(here[:, :LANES] + following)
        hidden.append(jax.nn.gelu(jnp.concatenate(per, 0)).astype(jnp.bfloat16))
    none = jnp.zeros(sko_ref.shape, jnp.float32)
    key_out = jnp.concatenate([sko_ref[...].astype(jnp.float32), none], 0).astype(jnp.bfloat16)
    value_out = jnp.concatenate([none, svo_ref[...].astype(jnp.float32)], 0).astype(jnp.bfloat16)
    summed = dot_nt(hidden[0], key_out) + dot_nt(hidden[1], value_out)
    low = low_half((summaries, LANES))
    sc = sturns_ref[0]
    ss = sturns_ref[1]
    scos = jnp.where(low, sc * base_cos - ss * base_sin, 1.0)
    ssin = jnp.where(low, (ss * base_cos + sc * base_sin) * sign, 0.0)
    for g in range(groups):
        pair = turn(summed[g * summaries : (g + 1) * summaries, :], scos, ssin)
        pair = pair.astype(jnp.bfloat16)
        sumown[g] = pair
        sumbuf[g, pl.ds(pl.multiple_of(me * summaries, summaries), summaries), :] = pair
    for d in range(1, n):

        @pl.when(me + d < n)
        def _(d=d):
            sum_copy(d, me, me + d).start()

    for d in range(1, n):

        @pl.when(me - d >= 0)
        def _(d=d):
            sum_copy(d, me - d, me).wait_recv()

    total = n * summaries
    listed = chosen_vec.shape[2]
    qrows = per_group * BLK
    in_block = lax.broadcasted_iota(jnp.int32, (qrows, 1), 0) % BLK
    ends = lax.broadcasted_iota(jnp.int32, (1, total), 1) * CMP_STRIDE + CMP_LEN - 1
    per_chunk = blocks // 4

    def mix(q, pairs, visible):
        scores = jnp.where(visible, dot_nt(q, pairs), NEGATIVE_FILL)
        largest = jnp.max(scores, -1, keepdims=True)
        weights = jnp.where(visible, jnp.exp(scores - largest), 0.0)
        total_weight = jnp.sum(weights, -1, keepdims=True)
        return dot(weights.astype(jnp.bfloat16), pairs), total_weight

    def gate_column(b, first):
        gate = gates[pl.ds(pl.multiple_of(b * BLK, BLK), BLK), :]
        return jnp.concatenate(
            [gate[:, first + r : first + r + 1] for r in range(per_group)], 0
        )

    def compressed_block(b, _):
        pos = me * rows + b * BLK + in_block
        at = pl.ds(pl.multiple_of(b * qrows, qrows), qrows)
        for g in range(groups):
            mixed, weight = mix(qbuf[g, at, :], sumbuf[g], ends <= pos)
            inverse = gate_column(b, g * per_group) / jnp.maximum(weight, 1.0)
            compr[g, at, :] = mixed * inverse
        return 0

    lax.fori_loop(0, blocks, compressed_block, 0)

    loc_copy.wait()
    for d in range(1, n):

        @pl.when(me - d >= 0)
        def _(d=d):
            kv_copy(d, me - d, me).wait_recv()

    tile_lane = lax.broadcasted_iota(jnp.int32, (1, LANES), 1)

    def attend(target, first, count, dst):
        def block(i, _):
            b = target * per_chunk + first + i
            pos = me * rows + b * BLK + in_block
            at = pl.ds(pl.multiple_of(b * qrows, qrows), qrows)
            for g in range(groups):
                key_tiles = []
                for k in range(0, listed, LANES // BLK):
                    which = jnp.zeros((1, LANES), jnp.int32)
                    for e in range(LANES // BLK):
                        chosen = chosen_ref[g, b, k + e]
                        where = locmap[g, chosen]
                        gath[g, (k + e) * BLK : (k + e + 1) * BLK, :] = kvbuf[g, where]
                        which = jnp.where(tile_lane // BLK == e, chosen, which)
                    key_tiles.append(which * BLK + tile_lane % BLK)
                key_positions = jnp.concatenate(key_tiles, 1)
                mixed, weight = mix(qbuf[g, at, :], gath[g], key_positions <= pos)
                inverse = gate_column(b, heads + g * per_group) / weight
                both = compr[g, at, :] + mixed * inverse
                for r in range(0, per_group, 2):
                    joined = jnp.where(
                        low_half((BLK, LANES)),
                        pltpu.roll(both[r * BLK : (r + 1) * BLK], HD, 1),
                        both[(r + 1) * BLK : (r + 2) * BLK],
                    )
                    column = (g * per_group + r) * HD
                    dst[pl.ds(pl.multiple_of(i * BLK, BLK), BLK), column : column + LANES] = (
                        joined.astype(jnp.bfloat16)
                    )
            return 0

        lax.fori_loop(0, count, block, 0)

    tile = 512
    columns = wo.shape[1]

    def project(dst, mine, theirs, added):
        for at in range(0, columns, tile):
            piece = dot(mine[...], wo[:, at : at + tile])
            piece = piece + dot(theirs[...], wo_other[:, at : at + tile])
            for other in added:
                piece = piece + other[:, at : at + tile].astype(jnp.float32)
            dst[:, at : at + tile] = piece.astype(jnp.bfloat16)

    part = per_chunk // 2
    part_rows = part * BLK
    sends = []
    arrivals = []
    for h in range(2):
        span = pl.ds(h * part_rows, part_rows)
        attend(diagonal, h * part, part, blended.at[0, span])
        send = rs_copy(1 + h, blended.at[0, span], blended_got.at[0, span], partner)
        send.start()
        sends.append(send)
        attend(across, h * part, part, blended.at[1, span])
        if h == 0:
            for copy in load_o:
                copy.wait()
            weight_copy.wait_recv()
        send.wait_recv()
        project(part_b.at[span], blended.at[1, span], blended_got.at[0, span], [])
        send = rs_copy(3 + h, part_b.at[span], got_b.at[span], across)
        send.start()
        sends.append(send)
        arrivals.append(send)
    attend(partner, 0, per_chunk, blended.at[2])
    send = rs_copy(5, blended.at[2], blended_got.at[1], partner)
    send.start()
    sends.append(send)
    attend(tp, 0, per_chunk, blended.at[3])
    send.wait_recv()
    for arrival in arrivals:
        arrival.wait_recv()
    project(out_ref, blended.at[3], blended_got.at[1], [got_b])

    sends.append(weight_copy)
    for copy in sends:
        copy.wait_send()
    for d in range(1, n):

        @pl.when(me - d >= 0)
        def _(d=d):
            slot_copy(d, me, me - d).wait_send()

        @pl.when(me + d < n)
        def _(d=d):
            kv_copy(d, me, me + d).wait_send()
            sum_copy(d, me, me + d).wait_send()

    @pl.when(me > 0)
    def _():
        halo_copy(me - 1).wait_send()


def rotary_constants(rows, n):
    inverse = ROTARY_BASE ** (-np.arange(HD // 2) / (HD // 2))
    lanes = np.tile(inverse, LANES // (HD // 2))[None, :]

    def table(positions):
        angles = np.asarray(positions, np.float64)[:, None] * lanes
        return np.stack([np.cos(angles), np.sin(angles)]).astype(np.float32)

    local = table(np.arange(rows))
    bases = table(np.arange(n) * rows).transpose(1, 0, 2)
    ends = table(np.arange(rows // CMP_STRIDE) * CMP_STRIDE + CMP_LEN - 1)
    return local, bases, ends


def fused(n, *args):
    (
        tokens,
        wq,
        wck,
        wcv,
        wsk,
        wsv,
        ski,
        sko,
        svi,
        svo,
        gate_weight,
        wo,
        chosen,
    ) = args
    rows, depth = tokens.shape
    groups = wck.shape[1] // HD
    per_group = wq.shape[1] // wck.shape[1]
    heads = groups * per_group
    blocks = rows // BLK
    listed = chosen.shape[2]
    every = n * blocks
    gate = gate_weight.transpose(0, 2, 1)
    local, bases, ends = rotary_constants(rows, n)
    chunk = rows // 4
    bf = jnp.bfloat16
    hbm = pl.BlockSpec(memory_space=pl.ANY)
    vmem = pl.BlockSpec(memory_space=pltpu.VMEM)
    wide = CAP * BLK
    summaries = rows // CMP_STRIDE
    part = pltpu.VMEM((chunk, wo.shape[1]), bf)
    dma = pltpu.SemaphoreType.DMA
    return pl.pallas_call(
        functools.partial(layer_kernel, n, groups, per_group),
        out_shape=jax.ShapeDtypeStruct((chunk, wo.shape[1]), bf),
        in_specs=[pl.BlockSpec(memory_space=pltpu.SMEM), vmem]
        + [hbm] * 8
        + [vmem] * 3
        + [hbm]
        + [vmem] * 3,
        out_specs=vmem,
        scratch_shapes=[
            pltpu.VMEM((rows, depth), bf),
            pltpu.VMEM((depth, heads * HD), bf),
            pltpu.VMEM((depth, 2 * LANES), bf),
            pltpu.VMEM((depth, 2 * LANES), bf),
            pltpu.VMEM((CMP_STRIDE * HD, 2 * LANES), bf),
            pltpu.VMEM((CMP_STRIDE * HD, 2 * LANES), bf),
            pltpu.VMEM(wo.shape, bf),
            pltpu.VMEM(wo.shape, bf),
            pltpu.VMEM((8, every), jnp.float32),
            pltpu.VMEM((8, every), jnp.int32),
            pltpu.SMEM((8, every), jnp.int32),
            pltpu.VMEM((n, 8, every), jnp.float32),
            pltpu.VMEM((groups, rows, LANES), bf),
            pltpu.VMEM((n, groups, CAP, BLK, LANES), bf),
            pltpu.VMEM((groups, n * CAP + blocks, BLK, LANES), bf),
            pltpu.VMEM((2, rows, LANES), jnp.float32),
            pltpu.VMEM((8, LANES), jnp.float32),
            pltpu.VMEM((8, LANES), jnp.float32),
            pltpu.VMEM((groups, summaries, LANES), bf),
            pltpu.VMEM((groups, n * summaries, LANES), bf),
            pltpu.VMEM((groups, rows * per_group, LANES), bf),
            pltpu.VMEM((rows, 2 * heads), jnp.float32),
            pltpu.VMEM((groups, listed * BLK, LANES), bf),
            pltpu.VMEM((groups, rows * per_group, LANES), jnp.float32),
            pltpu.VMEM((4, chunk, heads * HD), bf),
            pltpu.VMEM((2, chunk, heads * HD), bf),
            part,
            part,
            dma((11,)),
            dma((n,)),
            dma((n,)),
            dma((n,)),
            dma((n,)),
            dma((n,)),
            dma((n,)),
            dma(()),
            dma(()),
            dma((6,)),
            dma((6,)),
            dma(()),
        ],
        compiler_params=pltpu.CompilerParams(
            collective_id=0, has_side_effects=True, vmem_limit_bytes=60 * 1024 * 1024
        ),
        name="layer",
    )(chosen, chosen, tokens, wq, wck, wcv, wsk, wsv, ski, svi, sko.T, svo.T, gate, wo, local, bases, ends)


def solution(mesh):
    n = mesh.shape["kv"]

    def one_device(*args):
        fits = args[2].shape[1] == LANES and mesh.shape["tp"] == 4
        return fused(n, *args) if fits else on_device(*args)

    return jax.shard_map(
        one_device,
        mesh=mesh,
        in_specs=(
            P("kv", None),
            P(None, "tp"),
            P(None, "tp"),
            P(None, "tp"),
            P(None, "tp"),
            P(None, "tp"),
            P(),
            P(),
            P(),
            P(),
            P(None, None, "tp"),
            P("tp", None),
            P("tp", "kv", None),
        ),
        out_specs=P(("kv", "tp"), None),
        check_vma=False,
    )
```

```python
import functools

import numpy as np
import jax
import jax.numpy as jnp
from jax import lax
from jax.experimental import pallas as pl
from jax.experimental.pallas import tpu as pltpu
from jax.sharding import PartitionSpec as P

HD = 64
CMP_LEN = 32
CMP_STRIDE = 16
BLK = 32
CAP = 4
LANES = 128


ROTARY_BASE = 10000.0
NEGATIVE_FILL = -1e30


def from_behind(block, axis, distance):
    devices = range(lax.axis_size(axis))
    route = [(i - distance, i) for i in devices if i - distance in devices]
    return lax.ppermute(block, axis, route)


def rotate(values, positions):
    halfway = values.shape[-1] // 2
    inverse = ROTARY_BASE ** (-jnp.arange(halfway, dtype=jnp.float32) / halfway)
    angles = positions.astype(jnp.float32)[:, None] * inverse[None, :]
    cosine_rows = jnp.cos(angles)[:, None, :]
    sine_rows = jnp.sin(angles)[:, None, :]
    former = values[..., :halfway]
    latter = values[..., halfway:]
    return jnp.concatenate(
        [former * cosine_rows - latter * sine_rows, latter * cosine_rows + former * sine_rows], -1
    )


def squeeze_windows(windows, weight_in, weight_out):
    total_windows = windows.shape[0]
    groups = windows.shape[2]
    head_width = windows.shape[3]
    flattened = windows.transpose(0, 2, 1, 3).reshape(total_windows * groups, CMP_LEN * head_width)
    hidden = jax.nn.gelu(jnp.dot(flattened, weight_in, preferred_element_type=jnp.float32)).astype(
        jnp.bfloat16
    )
    return jnp.dot(hidden, weight_out, preferred_element_type=jnp.float32).reshape(
        total_windows, groups, head_width
    )


def online_step(running, scores, visible, values):
    largest, summed, weighted = running
    updated = jnp.maximum(largest, jnp.max(jnp.where(visible, scores, NEGATIVE_FILL), -1))
    weights = jnp.where(visible, jnp.exp(scores - updated[..., None]), 0.0)
    shrink = jnp.exp(largest - updated)
    summed = summed * shrink + jnp.sum(weights, -1)
    weighted = weighted * shrink[..., None] + jnp.einsum(
        "grqk,kgd->grqd", weights.astype(jnp.bfloat16), values, preferred_element_type=jnp.float32
    )
    return (updated, summed, weighted)


def on_device(
    tokens,
    query_weight,
    chosen_key_weight,
    chosen_value_weight,
    summary_key_weight,
    summary_value_weight,
    squeeze_key_in,
    squeeze_key_out,
    squeeze_value_in,
    squeeze_value_out,
    gate_weight,
    output_weight,
    chosen_blocks,
):
    tok_rows = tokens.shape[0]
    heads_here = query_weight.shape[1] // HD
    groups_here = chosen_key_weight.shape[1] // HD
    per_group = heads_here // groups_here
    kv_rank = lax.axis_index("kv")
    offset = kv_rank * tok_rows
    positions = offset + jnp.arange(tok_rows, dtype=jnp.int32)
    queries = rotate(
        jnp.dot(tokens, query_weight, preferred_element_type=jnp.float32).reshape(
            tok_rows, heads_here, HD
        ),
        positions,
    )
    queries = queries.astype(jnp.bfloat16).reshape(tok_rows, groups_here, per_group, HD)
    chosen_keys = rotate(
        jnp.dot(tokens, chosen_key_weight, preferred_element_type=jnp.float32).reshape(
            tok_rows, groups_here, HD
        ),
        positions,
    ).astype(jnp.bfloat16)
    chosen_values = (
        jnp.dot(tokens, chosen_value_weight, preferred_element_type=jnp.float32)
        .astype(jnp.bfloat16)
        .reshape(tok_rows, groups_here, HD)
    )
    chosen_pairs = jnp.concatenate([chosen_keys, chosen_values], -1)
    raw_keys = (
        jnp.dot(tokens, summary_key_weight, preferred_element_type=jnp.float32)
        .astype(jnp.bfloat16)
        .reshape(tok_rows, groups_here, HD)
    )
    raw_values = (
        jnp.dot(tokens, summary_value_weight, preferred_element_type=jnp.float32)
        .astype(jnp.bfloat16)
        .reshape(tok_rows, groups_here, HD)
    )
    raw_pairs = jnp.concatenate([raw_keys, raw_values], -1)
    following = from_behind(raw_pairs[:CMP_STRIDE], "kv", -1)
    extended = jnp.concatenate([raw_pairs, following], 0)
    summary_count = tok_rows // CMP_STRIDE
    segments = extended.reshape(summary_count + 1, CMP_STRIDE, groups_here, 2 * HD)
    windows = jnp.concatenate([segments[:-1], segments[1:]], 1)
    summary_ends = (
        (kv_rank * summary_count + jnp.arange(summary_count, dtype=jnp.int32)) * CMP_STRIDE
        + CMP_LEN
        - 1
    )
    summary_keys = rotate(
        squeeze_windows(windows[..., :HD], squeeze_key_in, squeeze_key_out), summary_ends
    ).astype(jnp.bfloat16)
    summary_values = squeeze_windows(windows[..., HD:], squeeze_value_in, squeeze_value_out).astype(
        jnp.bfloat16
    )
    summaries = jnp.concatenate([summary_keys, summary_values], -1)
    scaling = HD ** (-0.5)
    starting = (
        jnp.full((groups_here, per_group, tok_rows), NEGATIVE_FILL, jnp.float32),
        jnp.zeros((groups_here, per_group, tok_rows), jnp.float32),
        jnp.zeros((groups_here, per_group, tok_rows, HD), jnp.float32),
    )
    portion = lax.all_gather(summaries, "kv", axis=0, tiled=True)
    length = portion.shape[0]
    ends = jnp.arange(length, dtype=jnp.int32) * CMP_STRIDE + CMP_LEN - 1
    scores = (
        jnp.einsum("qgrd,kgd->grqk", queries, portion[..., :HD], preferred_element_type=jnp.float32)
        * scaling
    )
    visible = (ends[None, :] <= positions[:, None])[None, None]
    folded = online_step(starting, scores, visible, portion[..., HD:])
    compressed = folded[2] / jnp.maximum(folded[1], 1.0)[..., None]
    block_count = tok_rows // BLK

    def span_step(running, stretch, leading):
        length = stretch.shape[0]
        key_positions = leading + jnp.arange(length, dtype=jnp.int32)
        listed = jnp.any(
            chosen_blocks[:, :, :, None] == (key_positions // BLK)[None, None, None, :], axis=2
        )
        listed = jnp.broadcast_to(
            listed[:, :, None, :], (groups_here, block_count, BLK, length)
        ).reshape(groups_here, tok_rows, length)
        visible = (listed & (key_positions[None, None, :] <= positions[None, :, None]))[:, None]
        scores = (
            jnp.einsum(
                "qgrd,kgd->grqk", queries, stretch[..., :HD], preferred_element_type=jnp.float32
            )
            * scaling
        )
        return online_step(running, scores, visible, stretch[..., HD:])

    def maybe_step(running, stretch, leading):

        def step_taken(carried):
            return span_step(carried, stretch, leading)

        def step_skipped(carried):
            return carried

        return lax.cond(leading <= offset + tok_rows - 1, step_taken, step_skipped, running)

    portion = lax.all_gather(chosen_pairs, "kv", axis=0, tiled=True)
    length = portion.shape[0]
    stretch_rows = tok_rows * 4

    def visit_span(number, carried):
        stretch = lax.dynamic_slice_in_dim(portion, number * stretch_rows, stretch_rows, 0)
        return maybe_step(carried, stretch, number * stretch_rows)

    folded_chosen = lax.fori_loop(0, length // stretch_rows, visit_span, starting)
    selected = folded_chosen[2] / folded_chosen[1][..., None]
    first_gates = jax.nn.sigmoid(
        jnp.dot(tokens, gate_weight[0], preferred_element_type=jnp.float32)
    )
    second_gates = jax.nn.sigmoid(
        jnp.dot(tokens, gate_weight[1], preferred_element_type=jnp.float32)
    )
    first_gates = first_gates.reshape(tok_rows, groups_here, per_group).transpose(1, 2, 0)[
        ..., None
    ]
    second_gates = second_gates.reshape(tok_rows, groups_here, per_group).transpose(1, 2, 0)[
        ..., None
    ]
    blended = (
        (first_gates * compressed + second_gates * selected)
        .transpose(2, 0, 1, 3)
        .reshape(tok_rows, heads_here * HD)
        .astype(jnp.bfloat16)
    )
    attended = lax.psum_scatter(
        jnp.dot(blended, output_weight, preferred_element_type=jnp.float32).astype(jnp.bfloat16),
        "tp",
        scatter_dimension=0,
        tiled=True,
    )
    return attended


def dot(a, b):
    return jnp.dot(a, b, preferred_element_type=jnp.float32)


def dot_nt(a, b):
    return lax.dot_general(a, b, (((1,), (1,)), ((), ())), preferred_element_type=jnp.float32)


def low_half(shape):
    return lax.broadcasted_iota(jnp.int32, shape, 1) < HD


def turn(x, cos, sin):
    quarter = HD // 2
    lane = lax.broadcasted_iota(jnp.int32, x.shape, 1)
    swapped = jnp.where(
        lane % HD < quarter, pltpu.roll(x, LANES - quarter, 1), pltpu.roll(x, quarter, 1)
    )
    return x * cos + swapped * sin


def pair_halves(a, b):
    low = low_half(a.shape)
    return jnp.where(low, a, pltpu.roll(b, HD, 1)), jnp.where(low, pltpu.roll(a, HD, 1), b)


def layer_kernel(
    n,
    groups,
    per_group,
    chosen_ref,
    chosen_vec,
    tokens_hbm,
    wq_hbm,
    wck_hbm,
    wcv_hbm,
    wsk_hbm,
    wsv_hbm,
    ski_hbm,
    svi_hbm,
    sko_ref,
    svo_ref,
    gate_ref,
    wo_hbm,
    turns_ref,
    bases_ref,
    sturns_ref,
    out_ref,
    tok,
    wq,
    wc,
    ws,
    wki,
    wvi,
    wo,
    wo_other,
    slots_ref,
    locs,
    locmap,
    slotbuf,
    kvc,
    kvstage,
    kvbuf,
    rawf,
    halo_out,
    halo_in,
    sumown,
    sumbuf,
    qbuf,
    gates,
    gath,
    compr,
    blended,
    blended_got,
    part_b,
    got_b,
    load_sem,
    slot_send,
    slot_recv,
    kv_send,
    kv_recv,
    sum_send,
    sum_recv,
    halo_send,
    halo_recv,
    rs_send,
    rs_recv,
    loc_sem,
):
    me = lax.axis_index("kv")
    tp = lax.axis_index("tp")
    rows = tok.shape[0]
    blocks = rows // BLK
    heads = groups * per_group
    depth = tok.shape[1]
    wide = CAP * BLK
    own_base = n * CAP
    summaries = rows // CMP_STRIDE
    half = wki.shape[0]
    partner = tp + 1 - 2 * (tp % 2)
    across = (tp + 2) % 4
    diagonal = partner + 2 - 4 * (partner // 2)

    loads = []

    def load(src, dst):
        copy = pltpu.make_async_copy(src, dst, load_sem.at[len(loads)])
        copy.start()
        loads.append(copy)
        return copy

    load_c = [
        load(tokens_hbm, tok),
        load(wck_hbm, wc.at[:, 0:LANES]),
        load(wcv_hbm, wc.at[:, LANES : 2 * LANES]),
    ]
    load_s = [
        load(wsk_hbm, ws.at[:, 0:LANES]),
        load(wsv_hbm, ws.at[:, LANES : 2 * LANES]),
    ]
    load_i = [
        load(ski_hbm.at[0:half], wki.at[:, 0:LANES]),
        load(ski_hbm.at[half : 2 * half], wki.at[:, LANES : 2 * LANES]),
        load(svi_hbm.at[0:half], wvi.at[:, 0:LANES]),
        load(svi_hbm.at[half : 2 * half], wvi.at[:, LANES : 2 * LANES]),
    ]

    every = n * blocks
    lane = lax.broadcasted_iota(jnp.int32, (blocks, every), 1)
    query_block = me * blocks + lax.broadcasted_iota(jnp.int32, (blocks, 1), 0)
    row8 = lax.broadcasted_iota(jnp.int32, (8, every), 0)
    lane8 = lax.broadcasted_iota(jnp.int32, (8, every), 1)
    present = jnp.zeros((8, every), jnp.int32)
    for g in range(groups):
        asked = chosen_vec[g]
        asked = jnp.where(asked <= query_block, asked, -1)
        hit = jnp.where(asked[:, 0:1] == lane, 1, 0)
        for k in range(1, asked.shape[1]):
            hit = jnp.where(asked[:, k : k + 1] == lane, 1, hit)
        hit = jnp.max(hit, 0, keepdims=True)
        present = jnp.where(row8 == g, hit, present)
    slot = jnp.zeros((8, every), jnp.int32)
    for s in range(1, blocks):
        slot = slot + jnp.where(lane8 % blocks >= s, pltpu.roll(present, s, 1), 0)
    slots_ref[...] = jnp.where(present > 0, slot, -1).astype(jnp.float32)
    owner = lane8 // blocks
    locs[...] = jnp.where(
        owner == me,
        n * CAP + lane8 % blocks,
        jnp.where(owner < me, owner * CAP + jnp.minimum(slot, CAP - 1), n * CAP),
    )

    sumbuf[...] = jnp.zeros_like(sumbuf)
    halo_in[...] = jnp.zeros_like(halo_in)
    halo_out[...] = jnp.zeros_like(halo_out)

    barrier = pltpu.get_barrier_semaphore()
    for d in range(1, n):
        pl.semaphore_signal(
            barrier, inc=1, device_id={"kv": (me + d) % n}, device_id_type=pl.DeviceIdType.MESH
        )
    for other in (partner, across):
        pl.semaphore_signal(
            barrier, inc=1, device_id={"tp": other}, device_id_type=pl.DeviceIdType.MESH
        )
    pl.semaphore_wait(barrier, n + 1)

    loc_copy = pltpu.make_async_copy(locs, locmap, loc_sem)
    loc_copy.start()

    def slot_copy(d, src_rank, dst_rank):
        return pltpu.make_async_remote_copy(
            src_ref=slots_ref,
            dst_ref=slotbuf.at[src_rank],
            send_sem=slot_send.at[d],
            recv_sem=slot_recv.at[src_rank],
            device_id={"kv": dst_rank},
            device_id_type=pl.DeviceIdType.MESH,
        )

    def kv_copy(d, src_rank, dst_rank):
        return pltpu.make_async_remote_copy(
            src_ref=kvstage.at[d],
            dst_ref=kvbuf.at[:, pl.ds(src_rank * CAP, CAP)],
            send_sem=kv_send.at[d],
            recv_sem=kv_recv.at[src_rank],
            device_id={"kv": dst_rank},
            device_id_type=pl.DeviceIdType.MESH,
        )

    def sum_copy(d, src_rank, dst_rank):
        return pltpu.make_async_remote_copy(
            src_ref=sumown,
            dst_ref=sumbuf.at[:, pl.ds(src_rank * summaries, summaries), :],
            send_sem=sum_send.at[d],
            recv_sem=sum_recv.at[src_rank],
            device_id={"kv": dst_rank},
            device_id_type=pl.DeviceIdType.MESH,
        )

    def halo_copy(dst_rank):
        return pltpu.make_async_remote_copy(
            src_ref=halo_out,
            dst_ref=halo_in,
            send_sem=halo_send,
            recv_sem=halo_recv,
            device_id={"kv": dst_rank},
            device_id_type=pl.DeviceIdType.MESH,
        )

    def rs_copy(k, src, dst, target):
        return pltpu.make_async_remote_copy(
            src_ref=src,
            dst_ref=dst,
            send_sem=rs_send.at[k],
            recv_sem=rs_recv.at[k],
            device_id={"tp": target},
            device_id_type=pl.DeviceIdType.MESH,
        )

    for d in range(1, n):

        @pl.when(me - d >= 0)
        def _(d=d):
            slot_copy(d, me, me - d).start()

    load_q = [load(wq_hbm, wq)]
    load_o = [load(wo_hbm, wo)]
    weight_copy = rs_copy(0, wo_hbm, wo_other, partner)
    weight_copy.start()

    base_cos = bases_ref[me, 0:1, :]
    base_sin = bases_ref[me, 1:2, :]
    sign = jnp.where(
        lax.broadcasted_iota(jnp.int32, (1, LANES), 1) % HD < HD // 2, -1.0, 1.0
    )

    def tables(first, count):
        c = turns_ref[0, first : first + count, :]
        s = turns_ref[1, first : first + count, :]
        return c * base_cos - s * base_sin, (s * base_cos + c * base_sin) * sign

    for copy in load_c:
        copy.wait()
    step = 128
    for first in range(0, rows, step):
        both = dot(tok[first : first + step, :], wc[...])
        cos, sin = tables(first, step)
        keys = turn(both[:, 0:LANES], cos, sin)
        pairs = pair_halves(keys, both[:, LANES : 2 * LANES])
        for g in range(groups):
            pair = pairs[g].astype(jnp.bfloat16)
            kvc[g, first : first + step, :] = pair
            for k in range(step // BLK):
                kvbuf[g, own_base + first // BLK + k] = pair[k * BLK : (k + 1) * BLK, :]

    j = lax.broadcasted_iota(jnp.int32, (n * blocks, rows), 0)
    c = lax.broadcasted_iota(jnp.int32, (n * blocks, rows), 1)
    expand = jnp.where(j == me * blocks + c // BLK, 1.0, 0.0).astype(jnp.bfloat16)
    row = lax.broadcasted_iota(jnp.int32, (wide, rows), 0)
    col = lax.broadcasted_iota(jnp.int32, (wide, rows), 1)
    same_place = row % BLK == col % BLK
    row_slot = (row // BLK).astype(jnp.float32)
    for d in range(n - 1, 0, -1):

        @pl.when(me + d < n)
        def _(d=d):
            slot_copy(d, me + d, me).wait_recv()
            asked = dot(slotbuf[me + d].astype(jnp.bfloat16), expand)
            for g in range(groups):
                pick = jnp.where(same_place & (asked[g : g + 1, :] == row_slot), 1.0, 0.0)
                packed = dot(pick.astype(jnp.bfloat16), kvc[g]).astype(jnp.bfloat16)
                for k in range(CAP):
                    kvstage[d, g, k] = packed[k * BLK : (k + 1) * BLK, :]
            kv_copy(d, me, me + d).start()

    for copy in load_s:
        copy.wait()
    for first in range(0, rows, step):
        both = dot(tok[first : first + step, :], ws[...])
        rounded = both.astype(jnp.bfloat16).astype(jnp.float32)
        for kind in range(2):
            rawf[kind, first : first + step, :] = rounded[:, kind * LANES : (kind + 1) * LANES]
    for copy in load_i:
        copy.wait()
    layers = []
    for kind, weight in ((0, wki), (1, wvi)):
        pieces = [[] for _ in range(groups)]
        for p in range(0, CMP_STRIDE, 2):
            one = rawf[kind, pl.ds(p, summaries, stride=CMP_STRIDE), :]
            two = rawf[kind, pl.ds(p + 1, summaries, stride=CMP_STRIDE), :]
            for g, piece in enumerate(pair_halves(one, two)):
                pieces[g].append(piece.astype(jnp.bfloat16))
        segments = jnp.concatenate([jnp.concatenate(pieces[g], 1) for g in range(groups)], 0)
        layers.append(dot(segments, weight[...]))
    for kind in range(2):
        for g in range(groups):
            at = kind * groups + g
            halo_out[at : at + 1, :] = layers[kind][
                g * summaries : g * summaries + 1, LANES : 2 * LANES
            ]

    @pl.when(me > 0)
    def _():
        halo_copy(me - 1).start()

    for copy in load_q:
        copy.wait()
    scaling = HD**-0.5
    for first in range(0, rows, step):
        projected = dot(tok[first : first + step, :], wq[...])
        cos, sin = tables(first, step)
        cos = cos * scaling
        sin = sin * scaling
        for pair in range(heads // 2):
            turned = turn(projected[:, pair * LANES : (pair + 1) * LANES], cos, sin)
            low = low_half(turned.shape)
            for odd in range(2):
                head = 2 * pair + odd
                g, r = head // per_group, head % per_group
                part = pltpu.roll(turned, HD, 1) if odd else turned
                part = jnp.where(low, part, 0.0).astype(jnp.bfloat16)
                for k in range(step // BLK):
                    at = (first // BLK + k) * per_group * BLK + r * BLK
                    qbuf[g, at : at + BLK, :] = part[k * BLK : (k + 1) * BLK, :]
    gate_rows = jnp.concatenate([gate_ref[k].astype(jnp.float32) for k in range(2)], 0)
    gates[...] = jax.nn.sigmoid(dot_nt(tok[...], gate_rows.astype(jnp.bfloat16)))

    @pl.when(me < n - 1)
    def _():
        halo_copy(me).wait_recv()

    hidden = []
    last = lax.broadcasted_iota(jnp.int32, (summaries, LANES), 0) == summaries - 1
    for kind in range(2):
        per = []
        for g in range(groups):
            here = layers[kind][g * summaries : (g + 1) * summaries, :]
            at = kind * groups + g
            following = jnp.where(
                last, halo_in[at : at + 1, :], pltpu.roll(here[:, LANES:], summaries - 1, 0)
            )
            per.append(here[:, :LANES] + following)
        hidden.append(jax.nn.gelu(jnp.concatenate(per, 0)).astype(jnp.bfloat16))
    none = jnp.zeros(sko_ref.shape, jnp.float32)
    key_out = jnp.concatenate([sko_ref[...].astype(jnp.float32), none], 0).astype(jnp.bfloat16)
    value_out = jnp.concatenate([none, svo_ref[...].astype(jnp.float32)], 0).astype(jnp.bfloat16)
    summed = dot_nt(hidden[0], key_out) + dot_nt(hidden[1], value_out)
    low = low_half((summaries, LANES))
    sc = sturns_ref[0]
    ss = sturns_ref[1]
    scos = jnp.where(low, sc * base_cos - ss * base_sin, 1.0)
    ssin = jnp.where(low, (ss * base_cos + sc * base_sin) * sign, 0.0)
    for g in range(groups):
        pair = turn(summed[g * summaries : (g + 1) * summaries, :], scos, ssin)
        pair = pair.astype(jnp.bfloat16)
        sumown[g] = pair
        sumbuf[g, pl.ds(pl.multiple_of(me * summaries, summaries), summaries), :] = pair
    for d in range(1, n):

        @pl.when(me + d < n)
        def _(d=d):
            sum_copy(d, me, me + d).start()

    for d in range(1, n):

        @pl.when(me - d >= 0)
        def _(d=d):
            sum_copy(d, me - d, me).wait_recv()

    total = n * summaries
    listed = chosen_vec.shape[2]
    qrows = per_group * BLK
    in_block = lax.broadcasted_iota(jnp.int32, (qrows, 1), 0) % BLK
    ends = lax.broadcasted_iota(jnp.int32, (1, total), 1) * CMP_STRIDE + CMP_LEN - 1
    per_chunk = blocks // 4

    def mix(q, pairs, visible):
        scores = jnp.where(visible, dot_nt(q, pairs), NEGATIVE_FILL)
        largest = jnp.max(scores, -1, keepdims=True)
        weights = jnp.exp(scores - largest)
        total_weight = jnp.sum(weights, -1, keepdims=True)
        return dot(weights.astype(jnp.bfloat16), pairs), total_weight

    def gate_column(b, first):
        gate = gates[pl.ds(pl.multiple_of(b * BLK, BLK), BLK), :]
        return jnp.concatenate(
            [gate[:, first + r : first + r + 1] for r in range(per_group)], 0
        )

    def compressed_block(b, _):
        pos = me * rows + b * BLK + in_block
        at = pl.ds(pl.multiple_of(b * qrows, qrows), qrows)
        for g in range(groups):
            mixed, weight = mix(qbuf[g, at, :], sumbuf[g], ends <= pos)
            inverse = gate_column(b, g * per_group) / jnp.maximum(weight, 1.0)
            compr[g, at, :] = jnp.where(pos >= CMP_LEN - 1, mixed * inverse, 0.0)
        return 0

    lax.fori_loop(0, blocks, compressed_block, 0, unroll=2)

    loc_copy.wait()
    for d in range(1, n):

        @pl.when(me - d >= 0)
        def _(d=d):
            kv_copy(d, me - d, me).wait_recv()

    tile_lane = lax.broadcasted_iota(jnp.int32, (1, LANES), 1)

    def attend(target, first, count, dst):
        def blocks_pair(i, _):
            block(2 * i, 0)
            block(2 * i + 1, 1)
            return 0

        def block(i, slot):
            b = target * per_chunk + first + i
            pos = me * rows + b * BLK + in_block
            at = pl.ds(pl.multiple_of(b * qrows, qrows), qrows)
            for g in range(groups):
                key_tiles = []
                for k in range(0, listed, LANES // BLK):
                    which = jnp.zeros((1, LANES), jnp.int32)
                    for e in range(LANES // BLK):
                        chosen = chosen_ref[g, b, k + e]
                        where = locmap[g, chosen]
                        gath[slot, g, (k + e) * BLK : (k + e + 1) * BLK, :] = kvbuf[g, where]
                        which = jnp.where(tile_lane // BLK == e, chosen, which)
                    key_tiles.append(which * BLK + tile_lane % BLK)
                key_positions = jnp.concatenate(key_tiles, 1)
                mixed, weight = mix(qbuf[g, at, :], gath[slot, g], key_positions <= pos)
                inverse = gate_column(b, heads + g * per_group) / weight
                both = compr[g, at, :] + mixed * inverse
                for r in range(0, per_group, 2):
                    joined = jnp.where(
                        low_half((BLK, LANES)),
                        pltpu.roll(both[r * BLK : (r + 1) * BLK], HD, 1),
                        both[(r + 1) * BLK : (r + 2) * BLK],
                    )
                    column = (g * per_group + r) * HD
                    dst[pl.ds(pl.multiple_of(i * BLK, BLK), BLK), column : column + LANES] = (
                        joined.astype(jnp.bfloat16)
                    )

        if count == 2:
            blocks_pair(0, 0)
        else:
            lax.fori_loop(0, count // 2, blocks_pair, 0)

    tile = 512
    columns = wo.shape[1]

    def project(dst, mine, theirs, added):
        for at in range(0, columns, tile):
            piece = dot(mine[...], wo[:, at : at + tile])
            piece = piece + dot(theirs[...], wo_other[:, at : at + tile])
            for other in added:
                piece = piece + other[:, at : at + tile].astype(jnp.float32)
            dst[:, at : at + tile] = piece.astype(jnp.bfloat16)

    part = per_chunk // 2
    part_rows = part * BLK
    sends = []
    arrivals = []
    for h in range(2):
        span = pl.ds(h * part_rows, part_rows)
        attend(diagonal, h * part, part, blended.at[0, span])
        send = rs_copy(1 + h, blended.at[0, span], blended_got.at[0, span], partner)
        send.start()
        sends.append(send)
        attend(across, h * part, part, blended.at[1, span])
        if h == 0:
            for copy in load_o:
                copy.wait()
            weight_copy.wait_recv()
        send.wait_recv()
        project(part_b.at[span], blended.at[1, span], blended_got.at[0, span], [])
        send = rs_copy(3 + h, part_b.at[span], got_b.at[span], across)
        send.start()
        sends.append(send)
        arrivals.append(send)
    attend(partner, 0, per_chunk, blended.at[2])
    send = rs_copy(5, blended.at[2], blended_got.at[1], partner)
    send.start()
    sends.append(send)
    attend(tp, 0, per_chunk, blended.at[3])
    send.wait_recv()
    for arrival in arrivals:
        arrival.wait_recv()
    project(out_ref, blended.at[3], blended_got.at[1], [got_b])

    sends.append(weight_copy)
    for copy in sends:
        copy.wait_send()
    for d in range(1, n):

        @pl.when(me - d >= 0)
        def _(d=d):
            slot_copy(d, me, me - d).wait_send()

        @pl.when(me + d < n)
        def _(d=d):
            kv_copy(d, me, me + d).wait_send()
            sum_copy(d, me, me + d).wait_send()

    @pl.when(me > 0)
    def _():
        halo_copy(me - 1).wait_send()


def rotary_constants(rows, n):
    inverse = ROTARY_BASE ** (-np.arange(HD // 2) / (HD // 2))
    lanes = np.tile(inverse, LANES // (HD // 2))[None, :]

    def table(positions):
        angles = np.asarray(positions, np.float64)[:, None] * lanes
        return np.stack([np.cos(angles), np.sin(angles)]).astype(np.float32)

    local = table(np.arange(rows))
    bases = table(np.arange(n) * rows).transpose(1, 0, 2)
    ends = table(np.arange(rows // CMP_STRIDE) * CMP_STRIDE + CMP_LEN - 1)
    return local, bases, ends


def fused(n, *args):
    (
        tokens,
        wq,
        wck,
        wcv,
        wsk,
        wsv,
        ski,
        sko,
        svi,
        svo,
        gate_weight,
        wo,
        chosen,
    ) = args
    rows, depth = tokens.shape
    groups = wck.shape[1] // HD
    per_group = wq.shape[1] // wck.shape[1]
    heads = groups * per_group
    blocks = rows // BLK
    listed = chosen.shape[2]
    every = n * blocks
    gate = gate_weight.transpose(0, 2, 1)
    local, bases, ends = rotary_constants(rows, n)
    chunk = rows // 4
    bf = jnp.bfloat16
    hbm = pl.BlockSpec(memory_space=pl.ANY)
    vmem = pl.BlockSpec(memory_space=pltpu.VMEM)
    wide = CAP * BLK
    summaries = rows // CMP_STRIDE
    part = pltpu.VMEM((chunk, wo.shape[1]), bf)
    dma = pltpu.SemaphoreType.DMA
    return pl.pallas_call(
        functools.partial(layer_kernel, n, groups, per_group),
        out_shape=jax.ShapeDtypeStruct((chunk, wo.shape[1]), bf),
        in_specs=[pl.BlockSpec(memory_space=pltpu.SMEM), vmem]
        + [hbm] * 8
        + [vmem] * 3
        + [hbm]
        + [vmem] * 3,
        out_specs=vmem,
        scratch_shapes=[
            pltpu.VMEM((rows, depth), bf),
            pltpu.VMEM((depth, heads * HD), bf),
            pltpu.VMEM((depth, 2 * LANES), bf),
            pltpu.VMEM((depth, 2 * LANES), bf),
            pltpu.VMEM((CMP_STRIDE * HD, 2 * LANES), bf),
            pltpu.VMEM((CMP_STRIDE * HD, 2 * LANES), bf),
            pltpu.VMEM(wo.shape, bf),
            pltpu.VMEM(wo.shape, bf),
            pltpu.VMEM((8, every), jnp.float32),
            pltpu.VMEM((8, every), jnp.int32),
            pltpu.SMEM((8, every), jnp.int32),
            pltpu.VMEM((n, 8, every), jnp.float32),
            pltpu.VMEM((groups, rows, LANES), bf),
            pltpu.VMEM((n, groups, CAP, BLK, LANES), bf),
            pltpu.VMEM((groups, n * CAP + blocks, BLK, LANES), bf),
            pltpu.VMEM((2, rows, LANES), jnp.float32),
            pltpu.VMEM((8, LANES), jnp.float32),
            pltpu.VMEM((8, LANES), jnp.float32),
            pltpu.VMEM((groups, summaries, LANES), bf),
            pltpu.VMEM((groups, n * summaries, LANES), bf),
            pltpu.VMEM((groups, rows * per_group, LANES), bf),
            pltpu.VMEM((rows, 2 * heads), jnp.float32),
            pltpu.VMEM((2, groups, listed * BLK, LANES), bf),
            pltpu.VMEM((groups, rows * per_group, LANES), jnp.float32),
            pltpu.VMEM((4, chunk, heads * HD), bf),
            pltpu.VMEM((2, chunk, heads * HD), bf),
            part,
            part,
            dma((11,)),
            dma((n,)),
            dma((n,)),
            dma((n,)),
            dma((n,)),
            dma((n,)),
            dma((n,)),
            dma(()),
            dma(()),
            dma((6,)),
            dma((6,)),
            dma(()),
        ],
        compiler_params=pltpu.CompilerParams(
            collective_id=0, has_side_effects=True, vmem_limit_bytes=60 * 1024 * 1024
        ),
        name="layer",
    )(chosen, chosen, tokens, wq, wck, wcv, wsk, wsv, ski, svi, sko.T, svo.T, gate, wo, local, bases, ends)


def solution(mesh):
    n = mesh.shape["kv"]

    def one_device(*args):
        whole_blocks = args[0].shape[0] % (16 * BLK) == 0
        fits = args[2].shape[1] == LANES and mesh.shape["tp"] == 4 and whole_blocks
        return fused(n, *args) if fits else on_device(*args)

    return jax.shard_map(
        one_device,
        mesh=mesh,
        in_specs=(
            P("kv", None),
            P(None, "tp"),
            P(None, "tp"),
            P(None, "tp"),
            P(None, "tp"),
            P(None, "tp"),
            P(),
            P(),
            P(),
            P(),
            P(None, None, "tp"),
            P("tp", None),
            P("tp", "kv", None),
        ),
        out_specs=P(("kv", "tp"), None),
        check_vma=False,
    )
```
